512 devices in a mesh: sp: 32 (over z, core), tp: 16 (over y, x).
Axes of the slice: x: 4, y: 4, z: 16, core: 2. Of those that a mesh axis runs over, the one named last changes fastest.
Arguments:
- residual: bfloat16 [8192, 4096], P('sp', 'tp'), may hold values from -6 to 6
- pool_in: bfloat16 [8192, 2048], P('sp', 'tp'), may hold values from -6 to 6
- docs: int32 [8192], P('sp'), may hold values from 0 to 15, never falling along the last dimension, each value on 1 to 1024 neighbouring positions
- pool_weight: bfloat16 [16, 128, 128], P('tp'), may hold values from -0.5 to 0.5
- pool_gain: float32 [2048], P('tp'), may hold values from 0.1 to 1.9
- out_weight: bfloat16 [2048, 4096], P(None, 'tp'), may hold values from -0.125 to 0.125
- norm_gain: float32 [4096], replicated, may hold values from 0.1 to 1.9
- routes: int32 [8192, 2], P('sp'), may hold values from 0 to 31, all different within a row; in each aligned block of 256 rows (0 to 255, 256 to 511, ...) at most 24 rows name the same one
- route_weights: float32 [8192, 2], P('sp'), may hold values from 0.25 to 1
- w_gate: bfloat16 [32, 4096, 2048], P('sp', None, 'tp'), may hold values from -0.09375 to 0.09375
- w_up: bfloat16 [32, 4096, 2048], P('sp', None, 'tp'), may hold values from -0.09375 to 0.09375
- w_down: bfloat16 [32, 2048, 4096], P('sp', None, 'tp'), may hold values from -0.125 to 0.125
Outputs:
- layer_out: bfloat16 [8192, 4096], P('sp', 'tp')
The draws below stay inside these ranges and needn't reach their ends.
Inputs may be any that keep to these rules, and one draw needn't show every extreme that they name: `docs`: document numbers never fall along the sequence; each document has at most 1024 positions. `routes`: each token names 2 different experts; among the tokens of one index of sp (aligned blocks of 256 rows) no expert is named more than 24 times, a bound that some block reaches.
All inputs are finite; a program needn't handle non-finite values.
Results may differ from the reference program's by a relative error of at most 0.012.
Values may be sent and summed in bfloat16 or wider, within the bound.
No kernel may reach another device: no remote copies, remote signals or barrier semaphores. Data moves between devices by JAX's collectives and lax.ppermute only.
A program may use at most 64 MiB of HBM per device.

```python
import math
import jax
import jax.numpy as jnp
import numpy as np
from jax import lax

D = 4096
DFF = 2048
GD = 128
POOL_GROUPS = 16
TOPK = 2
TOK_DEV = 256
POOL_WIDTH = 2048
EXPERTS = 32
TOKENS = 8192
CAP = 24
DOCS = 16
DOC_MOST = 1024
N_SP = 32


def steps_of(stream_key, dims, split, least, top_value):
    factor_of, own = 1.0, jax.random.fold_in(stream_key, 6)
    for axis_at, parts in split:
        heights = jnp.exp(jax.random.uniform(jax.random.fold_in(own, axis_at), (parts,), jnp.float32, least / len(split), top_value / len(split)))
        factor_of = factor_of * jnp.repeat(heights, dims[axis_at] // parts).reshape([-1 if axis == axis_at else 1 for axis in range(len(dims))])
    return factor_of


def length_profile(number_of, total, most, slope):
    loads = [(1 << 20) // math.isqrt(rank ** slope) + 1 for rank in range(2, number_of + 1)]
    spare, given = total - most - (number_of - 1), [1] * (number_of - 1)
    while spare > 0:
        movable = [i for i in range(number_of - 1) if given[i] < most]
        whole, remaining = sum([loads[i] for i in movable]), spare
        for i in movable:
            extra = min(most - given[i], max(1, remaining * loads[i] // whole), spare)
            given[i] = given[i] + extra
            spare = spare - extra
    return np.array([most] + given)


def uneven_parts(key, count, total, bound, lean):
    if count == 2:
        one = jax.random.randint(key, (), max(1, total - bound), min(bound, total - 1) + 1)
        return jnp.stack([one, total - one])
    sizes = jnp.asarray(length_profile(count, total, bound, lean), jnp.int32)
    twos = (count - 1) // 2
    giver, sink = sizes[1:1 + 2 * twos:2], sizes[2:2 + 2 * twos:2]
    room = jnp.minimum(giver - 1, bound - sink)
    moved = jax.random.randint(jax.random.fold_in(key, 1), (twos,), 0, 1 << 20) % (room + 1)
    sizes = sizes.at[1:1 + 2 * twos:2].set(giver - moved).at[2:2 + 2 * twos:2].set(sink + moved)
    return sizes[jax.random.permutation(jax.random.fold_in(key, 2), count)]


def routed_block(rng, own, number, rows, amount, top, limit, slope):
    ranking = jax.random.permutation(rng, amount)
    crowded, common = load_shares(amount, rows * top, limit, slope, True), load_shares(amount, rows * top, limit, slope, False)
    places = jnp.arange(amount)

    def named(tallies, turn):
        used = int((tallies > 0).sum())
        fixed = max(1, used // 4)
        moved = fixed + (places - fixed + turn * (used - fixed)) % max(1, amount - fixed)
        return jnp.zeros((amount,), jnp.int32).at[ranking[jnp.where(places < fixed, places, moved)]].set(jnp.asarray(tallies, jnp.int32))

    tallies = jnp.where(number % 4 == 0, named(crowded, number // 4), named(common, number - number // 4 - 1))
    mixed = jax.random.permutation(jax.random.fold_in(own, 3), amount)
    giver, sink = mixed[0:amount // 2 * 2:2], mixed[1:amount // 2 * 2:2]
    slack = jnp.minimum(tallies[giver] - 1, limit - tallies[sink]) // 2
    slack = jnp.where((giver == ranking[0]) | (sink == ranking[0]) | (tallies[sink] == 0), 0, jnp.maximum(slack, 0))
    moved = jax.random.randint(jax.random.fold_in(own, 4), (amount // 2,), 0, 1 << 20) % (slack + 1)
    tallies = tallies.at[giver].add(-moved).at[sink].add(moved)
    items = jnp.searchsorted(jnp.cumsum(tallies), jnp.arange(rows * top), side="right").astype(jnp.int32)
    grid = items.reshape(top, rows).T
    grid = grid[jax.random.permutation(jax.random.fold_in(own, 1), rows)]
    turn = jax.random.randint(jax.random.fold_in(own, 2), (rows, 1), 0, top)
    return jnp.take_along_axis(grid, (jnp.arange(top)[None, :] + turn) % top, axis=1)


def load_shares(number_of, total, reach, slope, full):
    portions = [(1 << 20) // math.isqrt(standing ** slope) + 1 for standing in range(1, number_of + 1)]
    largest = reach if full else min(reach, max(-(-total // number_of), total * portions[0] // sum(portions)))
    least = 1 if total - largest >= number_of - 1 else 0
    holding, spare = [largest] + [least] * (number_of - 1), total - largest - least * (number_of - 1)
    while spare > 0:
        candidates = [i for i in range(1, number_of) if holding[i] < largest] or [i for i in range(1, number_of) if holding[i] < reach]
        whole, budget = sum([portions[i] for i in candidates]), spare
        for i in candidates:
            addition = min(reach - holding[i], max(1, budget * portions[i] // whole), spare)
            holding[i] = holding[i] + addition
            spare = spare - addition
    return np.array(holding)


def bell_draw(own_key, extent, deviation, most, shards=(), held_as=jnp.bfloat16):
    drawn = deviation * jax.random.normal(own_key, extent, jnp.float32)
    if shards:
        drawn = drawn * steps_of(own_key, extent, shards, -0.22, 0.18)
    return jnp.clip(drawn, -most, most).astype(held_as)


def setup_inputs(seed: int = 0) -> dict:
    key_list = jax.random.split(jax.random.key(seed), 13)
    residual = bell_draw(key_list[0], (TOKENS, D), 1.0, 6.0, ((0, 32), (1, 16)))
    pool_in = bell_draw(key_list[1], (TOKENS, POOL_WIDTH), 1.0, 6.0, ((0, 32), (1, 16)))
    docs = jnp.searchsorted(jnp.cumsum(uneven_parts(key_list[2], DOCS, TOKENS, DOC_MOST, 1)), jnp.arange(TOKENS), side="right").astype(jnp.int32)
    pool_weight = bell_draw(key_list[3], (POOL_GROUPS, GD, GD), GD ** -0.5, 0.5, ((0, 16),))
    pool_gain = jnp.clip(1.0 + 0.18 * jax.random.normal(key_list[4], (POOL_WIDTH,), jnp.float32), 0.1, 1.9)
    out_weight = bell_draw(key_list[5], (POOL_WIDTH, D), POOL_WIDTH ** -0.5, 0.125, ((1, 16),))
    norm_gain = jnp.clip(1.0 + 0.18 * jax.random.normal(key_list[6], (D,), jnp.float32), 0.1, 1.9)
    routes_keys = jax.random.split(jax.random.fold_in(key_list[7], 1), TOKENS // TOK_DEV)
    routes_turns = jax.random.permutation(jax.random.fold_in(key_list[7], 3), TOKENS // TOK_DEV)
    routes = jax.vmap(lambda own, number: routed_block(jax.random.fold_in(key_list[7], 2), own, number, TOK_DEV, EXPERTS, TOPK, CAP, 1))(routes_keys, routes_turns).reshape((TOKENS, TOPK))
    route_weights = jnp.clip(0.25 + 0.75 * jax.random.uniform(key_list[8], (TOKENS, TOPK), jnp.float32) ** steps_of(key_list[8], (TOKENS, TOPK), ((0, 32),), -0.2, 0.2), 0.25, 1.0)
    w_gate = bell_draw(key_list[9], (EXPERTS, D, DFF), D ** -0.5, 0.09375, ((0, 32), (2, 16)))
    w_up = bell_draw(key_list[10], (EXPERTS, D, DFF), D ** -0.5, 0.09375, ((0, 32), (2, 16)))
    w_down = bell_draw(key_list[11], (EXPERTS, DFF, D), DFF ** -0.5, 0.125, ((0, 32), (2, 16)))
    return {"residual": residual, "pool_in": pool_in, "docs": docs, "pool_weight": pool_weight, "pool_gain": pool_gain, "out_weight": out_weight, "norm_gain": norm_gain, "routes": routes, "route_weights": route_weights, "w_gate": w_gate, "w_up": w_up, "w_down": w_down}


EPS = 1e-06

def pool_mix(pool_in, docs, pool_weight, pool_gain):
    length = pool_in.shape[0]
    values = pool_in.astype(jnp.float32)
    places = jnp.arange(length)
    group_of = jnp.arange(POOL_WIDTH) // GD
    span = 2 ** (1 + group_of % 4)
    totals = jnp.zeros((length, POOL_WIDTH), jnp.float32)
    counts = jnp.zeros((length, POOL_WIDTH), jnp.float32)
    for offset in range(16):
        shifted = jnp.pad(values, ((offset, 0), (0, 0)))[:length]
        prior = jnp.pad(docs, (offset, 0))[:length]
        same = ((places >= offset) & (prior == docs)).astype(jnp.float32)[:, None]
        inside = (offset < span).astype(jnp.float32)[None, :]
        weight = same * inside
        totals = totals + weight * shifted
        counts = counts + weight
    diff = (totals / counts - values).astype(jnp.bfloat16)
    mixed = jnp.einsum('tgc,gcd->tgd', diff.reshape(length, POOL_GROUPS, GD).astype(jnp.float32), pool_weight.astype(jnp.float32))
    return (mixed.reshape(length, POOL_WIDTH) * pool_gain).astype(jnp.bfloat16)

def expert_apply(packed):
    rows, gate_w, up_w, down_w = packed
    gate = jnp.dot(rows, gate_w, preferred_element_type=jnp.float32)
    up = jnp.dot(rows, up_w, preferred_element_type=jnp.float32)
    act = (jax.nn.silu(gate) * up).astype(jnp.bfloat16)
    return jnp.dot(act, down_w, preferred_element_type=jnp.float32).astype(jnp.bfloat16)

def reference(residual, pool_in, docs, pool_weight, pool_gain, out_weight, norm_gain, routes, route_weights, w_gate, w_up, w_down):
    pooled = pool_mix(pool_in, docs, pool_weight, pool_gain)
    proj = jnp.dot(pooled, out_weight, preferred_element_type=jnp.float32)
    updated = (residual.astype(jnp.float32) + proj).astype(jnp.bfloat16)
    upf = updated.astype(jnp.float32)
    normed = (upf * lax.rsqrt(lax.optimization_barrier(jnp.mean(upf * upf, axis=1, keepdims=True)) + EPS) * norm_gain).astype(jnp.bfloat16)
    ids = routes.reshape(N_SP, TOK_DEV * TOPK)
    onehot = (ids[:, :, None] == jnp.arange(EXPERTS)[None, None, :]).astype(jnp.int32)
    rank = lax.optimization_barrier(jnp.sum(onehot * (jnp.cumsum(onehot, axis=1) - 1), axis=2))
    blocks = jnp.arange(N_SP)[:, None]
    flat = (ids * (N_SP * CAP) + blocks * CAP + rank).reshape(-1).astype(jnp.int32)
    source = (blocks * TOK_DEV + jnp.arange(TOK_DEV * TOPK)[None, :] // TOPK).reshape(-1).astype(jnp.int32)
    buffer = jnp.zeros((EXPERTS * N_SP * CAP, D), jnp.bfloat16).at[flat].set(normed[source])
    results = lax.map(expert_apply, (buffer.reshape(EXPERTS, N_SP * CAP, D), w_gate, w_up, w_down))
    picked = results.reshape(EXPERTS * N_SP * CAP, D)[flat].reshape(TOKENS, TOPK, D)
    combined = upf + lax.optimization_barrier(jnp.sum(route_weights[:, :, None] * picked.astype(jnp.float32), axis=1))
    return combined.astype(jnp.bfloat16)
```

```python
import jax
import jax.numpy as jnp
from jax import lax
from jax.sharding import Mesh
from jax.sharding import PartitionSpec as P

TOPK = 2
SP = ("z", "c")
TP = ("y", "x")
EPS = 1e-06
F32 = jnp.float32
BF16 = jnp.bfloat16


def a2a(blocks, axis):
    return lax.all_to_all(blocks, axis, 0, 0, tiled=True)


def to_all(block, axis, size):
    return a2a(jnp.broadcast_to(block[None], (size, *block.shape)), axis)


def pool(pool_in, docs, pool_weight, pool_gain):
    length, width = pool_in.shape
    sp_index = lax.axis_index(SP)
    group = lax.axis_index(TP)
    size = lax.axis_size(SP)
    reach = 15
    tail = docs[length - 16 :].astype(BF16)
    edge = jnp.concatenate([pool_in[length - reach :], jnp.pad(tail, (0, width - 16))[None]], axis=0)
    prev = lax.ppermute(edge, SP, [(i, i + 1) for i in range(size - 1)])
    extended = jnp.concatenate([prev[:reach], pool_in], axis=0).astype(F32)
    own_docs = docs.astype(F32)
    ext_docs = jnp.concatenate([prev[reach, 1:16].astype(F32), own_docs])
    places = sp_index * length + jnp.arange(length)
    span = 2 ** (1 + group % 4)
    totals = jnp.zeros((length, width), F32)
    counts = jnp.zeros((length,), F32)
    for offset in range(16):
        shifted = extended[reach - offset : reach - offset + length]
        prior = ext_docs[reach - offset : reach - offset + length]
        same = ((places >= offset) & (prior == own_docs) & (offset < span)).astype(F32)
        totals = totals + same[:, None] * shifted
        counts = counts + same
    diff = (totals / counts[:, None] - extended[reach:]).astype(BF16)
    mixed = jnp.dot(diff, pool_weight[0], preferred_element_type=F32)
    return (mixed * pool_gain).astype(BF16)


def weights_of(w_gate, w_up, w_down, gain, gather, scatter):
    both = jnp.concatenate([w_gate, w_up], axis=1)
    if gather == "x":
        first = both.reshape(4, 1024, 256)
        own_gain = lax.dynamic_slice_in_dim(gain.reshape(4, 1024), lax.axis_index("y"), 1, 0)[0]
        second = w_down.reshape(4, 4, 128, 256).transpose(1, 0, 2, 3).reshape(4, 512, 256)
    else:
        first = both.reshape(4, 4, 256, 256).transpose(1, 0, 2, 3).reshape(4, 1024, 256)
        own_gain = lax.dynamic_slice_in_dim(gain.reshape(4, 4, 256), lax.axis_index("x"), 1, 1).reshape(1024)
        second = w_down.reshape(4, 512, 256)
    first = a2a(first, scatter)
    second = a2a(second, gather)
    first = (first.astype(F32) * own_gain[None, :, None]).astype(BF16)
    return first, second


def experts(rows, first, second, gather, scatter):
    count = rows.shape[0]
    got = to_all(rows, gather, 4)
    squares = jnp.sum(jnp.square(got.astype(F32)), axis=(0, 2))
    part = jnp.einsum("grf,sgfh->srh", got, first.reshape(4, 4, 256, 256), preferred_element_type=F32)
    parts = a2a(part.astype(BF16), scatter)
    all_squares = jnp.sum(to_all(squares.reshape(1, count), scatter, 4), axis=(0, 1))
    scale = lax.rsqrt(all_squares / 4096 + EPS)[:, None]
    both = jnp.sum(parts.astype(F32), axis=0) * scale
    gate, up = both[:, :128], both[:, 128:]
    act = (jax.nn.silu(gate) * up).astype(BF16)
    acts = to_all(act, scatter, 4)
    part = jnp.einsum("hrk,ghkf->grf", acts, second.reshape(4, 4, 128, 256), preferred_element_type=F32)
    parts = a2a(part.astype(BF16), gather)
    return jnp.sum(parts.astype(F32), axis=0).astype(BF16)


def shards(
    residual, pool_in, docs, pool_weight, pool_gain, out_weight, norm_gain, routes, route_weights, w_gate, w_up, w_down
):
    length, cols = residual.shape
    n_z, n_c = lax.axis_size("z"), lax.axis_size("c")
    n_exp = n_z * n_c
    cap = length * TOPK * 3 // (2 * n_exp)
    slots = n_exp * cap
    pooled = pool(pool_in, docs, pool_weight, pool_gain)
    ids = routes.reshape(-1)
    onehot = (ids[:, None] == jnp.arange(n_exp)[None, :]).astype(jnp.int32)
    rank = jnp.sum(onehot * (jnp.cumsum(onehot, axis=0) - 1), axis=1)
    place = (((ids % n_c) * n_z + ids // n_c) * cap + rank).reshape(length, TOPK)
    places = jnp.arange(slots)
    take = (place[:, 0][None, :] == places[:, None]) | (place[:, 1][None, :] == places[:, None])
    low = jnp.where(place[:, 0][:, None] == places[None, :], route_weights[:, 0][:, None], 0.0)
    mix = low + jnp.where(place[:, 1][:, None] == places[None, :], route_weights[:, 1][:, None], 0.0)
    mix_high = mix.astype(BF16)
    mix_low = (mix - mix_high.astype(F32)).astype(BF16)

    weights = {
        "x": weights_of(w_gate[0], w_up[0], w_down[0], norm_gain, "x", "y"),
        "y": weights_of(w_gate[0], w_up[0], w_down[0], norm_gain, "y", "x"),
    }

    pooled_all = to_all(pooled, TP, 16)
    proj = jnp.einsum("gtc,gcd->td", pooled_all, out_weight.reshape(16, 128, cols), preferred_element_type=F32)
    updated = (residual.astype(F32) + proj).astype(BF16)

    send = jnp.dot(take.astype(BF16), updated, preferred_element_type=F32).astype(BF16)
    send = a2a(send.reshape(n_c, n_z * cap, cols), "c")
    made = []
    for half, (gather, scatter) in enumerate((("x", "y"), ("y", "x"))):
        rows = a2a(send[half].reshape(n_z, cap, cols), "z").reshape(n_z * cap, cols)
        out = experts(rows, *weights[gather], gather, scatter)
        made.append(a2a(out.reshape(n_z, cap, cols), "z").reshape(n_z * cap, cols))
    back = a2a(jnp.stack(made), "c").reshape(slots, cols)
    summed = jnp.dot(mix_high, back, preferred_element_type=F32) + jnp.dot(
        mix_low, back, preferred_element_type=F32
    )
    return (updated.astype(F32) + summed).astype(BF16)


def solution(mesh):
    torus = Mesh(mesh.devices.reshape(-1, 2, 4, 4), ("z", "c", "y", "x"))
    in_specs = (
        P(SP, TP),
        P(SP, TP),
        P(SP),
        P(TP, None, None),
        P(TP),
        P(None, TP),
        P(),
        P(SP, None),
        P(SP, None),
        P(SP, None, TP),
        P(SP, None, TP),
        P(SP, None, TP),
    )
    return jax.shard_map(shards, mesh=torus, in_specs=in_specs, out_specs=P(SP, TP), check_vma=False)
```

```python
import functools

import jax
import jax.numpy as jnp
import numpy as np
from jax import lax
from jax.experimental import pallas as pl
from jax.experimental.pallas import tpu as pltpu
from jax.sharding import Mesh
from jax.sharding import PartitionSpec as P


TOPK = 2
SP = ("z", "c")
TP = ("y", "x")
PLANE = ("c", "y", "x")
EPS = 1e-06
F32 = jnp.float32
BF16 = jnp.bfloat16
VMEM_BYTES = 20 * 2**20


def blocks_of(shift):
    return [
        [(2 * v + shift + i) % 4 * 4 + (2 * h + shift + j) % 4 for i in (0, 1) for j in (0, 1)]
        for v in (0, 1)
        for h in (0, 1)
    ]


GATHER = [blocks_of(0), blocks_of(1)]
SCATTER = [blocks_of(1), blocks_of(0)]


def both_cores(groups):
    return groups[0] + [[16 + m for m in group] for group in groups[1]]


def group_with(groups, member):
    return next(group for group in groups if member in group)


def turned_back(group, member):
    at = group.index(member)
    return [group[(at - by) % 4] for by in range(4)]


def tables():
    table = np.zeros((2, 16, 56), np.int32)
    for core in range(2):
        for me in range(16):
            gather, scatter = group_with(GATHER[core], me), group_with(SCATTER[core], me)
            p, q = scatter.index(me), gather.index(me)
            features, hidden, channels = [], [], []
            for by in range(4):
                peer = scatter[(p + by) % 4]
                features += turned_back(group_with(GATHER[core], peer), peer)
                peer = gather[(q + by) % 4]
                hidden += turned_back(group_with(SCATTER[core], peer), peer)
                peer = scatter[(p - by) % 4]
                channels += turned_back(group_with(GATHER[core], peer), peer)
            table[core, me, :52] = features + hidden + turned_back(gather, me) + channels
    return table


FEATURES, HIDDEN, GAINS, CHANNELS = 0, 16, 32, 36


def turns(blocks, groups, sign=1):
    got = [blocks[0]]
    for by in range(1, 4):
        pairs = [(g[i], g[(i + sign * by) % 4]) for g in both_cores(groups) for i in range(4)]
        got.append(lax.ppermute(blocks[by], PLANE, pairs))
    return got


def shape(*dims, dtype=BF16):
    return jax.ShapeDtypeStruct(dims, dtype)


def call(kernel, outs, *args, flops, scratch=()):
    single = len(outs) == 1
    moved = sum(a.size * a.dtype.itemsize for a in (*args, *outs))
    vmem = pl.BlockSpec(memory_space=pltpu.VMEM)
    return pl.pallas_call(
        kernel,
        out_shape=outs[0] if single else tuple(outs),
        in_specs=[pl.BlockSpec(memory_space=pltpu.SMEM) if a.dtype == jnp.int32 else vmem for a in args],
        out_specs=vmem if single else (vmem,) * len(outs),
        scratch_shapes=list(scratch),
        compiler_params=pltpu.CompilerParams(vmem_limit_bytes=VMEM_BYTES),
        cost_estimate=pl.CostEstimate(flops=flops, bytes_accessed=moved, transcendentals=0),
    )(*args)


def cut_first(where, gate, up, *outs):
    for by in range(4):
        for i in range(4):
            block = where[FEATURES + 4 * by + i]
            src = pl.ds(pl.multiple_of(block * 256, 256), 256)
            outs[by][pl.ds(256 * i, 256), pl.ds(0, 128)] = gate[src, :]
            outs[by][pl.ds(256 * i, 256), pl.ds(128, 128)] = up[src, :]


def cut_second(where, down, *outs):
    for by in range(4):
        for i in range(4):
            block = where[HIDDEN + 4 * by + i]
            outs[by][pl.ds(128 * i, 128), :] = down[pl.ds(pl.multiple_of(block * 128, 128), 128), :]


def project(where, p0, p1, p2, p3, weight, residual, out):
    total = residual[...].astype(F32)
    for by, part in enumerate((p0, p1, p2, p3)):
        rows = [
            weight[pl.ds(pl.multiple_of(where[CHANNELS + 4 * by + i] * 128, 128), 128), :] for i in range(4)
        ]
        total = total + jnp.dot(part[...], jnp.concatenate(rows, axis=0), preferred_element_type=F32)
    out[...] = total.astype(BF16)


def gate_up(where, g0, g1, g2, g3, gain, w0, w1, w2, w3, o0, o1, o2, o3, rows):
    count = g0.shape[0]
    ones = jnp.ones((8, 256), BF16)
    tiles = count // 256
    outs = (o0, o1, o2, o3)
    for i in range(tiles):
        tile = pl.ds(256 * i, 256)
        total = jnp.zeros((8, 256), F32)
        for g, got in enumerate((g0, g1, g2, g3)):
            value = got[tile, :].astype(F32)
            rows[tile, pl.ds(256 * g, 256)] = (value * gain[pl.ds(where[GAINS + g], 1), :]).astype(BF16)
            square = value * value
            high = square.astype(BF16)
            low = (square - high.astype(F32)).astype(BF16)
            for part in (high, low):
                total = total + lax.dot_general(ones, part, (((1,), (1,)), ((), ())), preferred_element_type=F32)
        high = total.astype(BF16)
        low = (total - high.astype(F32)).astype(BF16)
        for out in outs:
            out[pl.ds(count + 2 * i, 1), :] = high[:1]
            out[pl.ds(count + 2 * i + 1, 1), :] = low[:1]
    for out, first in zip(outs, (w0, w1, w2, w3)):
        out[pl.ds(count + 2 * tiles, 8 - 2 * tiles), :] = jnp.zeros((8 - 2 * tiles, 256), BF16)
        for i in range(tiles):
            tile = pl.ds(256 * i, 256)
            out[tile, :] = jnp.dot(rows[tile, :], first[...], preferred_element_type=F32).astype(BF16)


def activate(p0, p1, p2, p3, out):
    count = out.shape[0]
    parts = (p0, p1, p2, p3)
    extra = jnp.concatenate([part[pl.ds(count, 8), :].astype(F32) for part in parts], axis=0)
    line = lax.broadcasted_iota(jnp.int32, (32, 128), 0) % 8
    for i in range(count // 256):
        tile = pl.ds(256 * i, 256)
        pick = ((line == 2 * i) | (line == 2 * i + 1)).astype(F32)
        total = lax.dot_general(extra, pick, (((0,), (0,)), ((), ())), preferred_element_type=F32)
        scale = lax.rsqrt(total / 4096 + EPS)
        gate = p0[tile, pl.ds(0, 128)].astype(F32)
        up = p0[tile, pl.ds(128, 128)].astype(F32)
        for part in parts[1:]:
            gate = gate + part[tile, pl.ds(0, 128)].astype(F32)
            up = up + part[tile, pl.ds(128, 128)].astype(F32)
        gate, up = gate * scale, up * scale
        out[tile, :] = (gate * jax.nn.sigmoid(gate) * up).astype(BF16)


def down_rows(a0, a1, a2, a3, w0, w1, w2, w3, o0, o1, o2, o3, rows):
    count = a0.shape[0]
    for h, act in enumerate((a0, a1, a2, a3)):
        rows[:, pl.ds(128 * h, 128)] = act[...]
    for out, second in zip((o0, o1, o2, o3), (w0, w1, w2, w3)):
        for i in range(count // 256):
            tile = pl.ds(256 * i, 256)
            out[tile, :] = jnp.dot(rows[tile, :], second[...], preferred_element_type=F32).astype(BF16)


def experts(arrived, first, second, where, gain):
    count = arrived.shape[0]
    got = turns([arrived] * 4, GATHER)
    parts = call(
        gate_up,
        [shape(count + 8, 256)] * 4,
        where,
        *got,
        gain,
        *first,
        flops=2**21 * count,
        scratch=[pltpu.VMEM((count, 1024), BF16)],
    )
    parts = turns(parts, SCATTER, -1)
    act = call(activate, [shape(count, 128)], *parts, flops=2**16 * count)
    acts = turns([act] * 4, SCATTER)
    parts = call(
        down_rows,
        [shape(count, 256)] * 4,
        *acts,
        *second,
        flops=2**20 * count,
        scratch=[pltpu.VMEM((count, 512), BF16)],
    )
    parts = turns(parts, GATHER, -1)
    return functools.reduce(jnp.add, [part.astype(F32) for part in parts]).astype(BF16)


def pool(pool_in, docs, pool_weight, pool_gain):
    length, width = pool_in.shape
    sp_index = lax.axis_index(SP)
    group = lax.axis_index(TP)
    size = lax.axis_size(SP)
    reach = 15
    tail = docs[length - 16 :].astype(BF16)
    edge = jnp.concatenate([pool_in[length - reach :], jnp.pad(tail, (0, width - 16))[None]], axis=0)
    prev = lax.ppermute(edge, SP, [(i, i + 1) for i in range(size - 1)])
    extended = jnp.concatenate([prev[:reach], pool_in], axis=0).astype(F32)
    own_docs = docs.astype(F32)
    ext_docs = jnp.concatenate([prev[reach, 1:16].astype(F32), own_docs])
    places = sp_index * length + jnp.arange(length)
    span = 2 ** (1 + group % 4)
    totals = jnp.zeros((length, width), F32)
    counts = jnp.zeros((length,), F32)
    for offset in range(16):
        shifted = extended[reach - offset : reach - offset + length]
        prior = ext_docs[reach - offset : reach - offset + length]
        same = ((places >= offset) & (prior == own_docs) & (offset < span)).astype(F32)
        totals = totals + same[:, None] * shifted
        counts = counts + same
    diff = (totals / counts[:, None] - extended[reach:]).astype(BF16)
    mixed = jnp.dot(diff, pool_weight[0], preferred_element_type=F32)
    return (mixed * pool_gain).astype(BF16)


def split(value):
    high = lax.reduce_precision(value, 8, 7)
    return high.astype(BF16), (value - high).astype(BF16)


def layer(
    residual, pool_in, docs, pool_weight, pool_gain, out_weight, norm_gain, routes, route_weights, w_gate, w_up, w_down
):
    length, cols = residual.shape
    n_exp = lax.axis_size(SP)
    cap = length * TOPK * 3 // (2 * n_exp)
    slots = n_exp * cap
    where = lax.dynamic_slice(
        jnp.asarray(tables()), (lax.axis_index("c"), lax.axis_index(TP), 0), (1, 1, 56)
    ).reshape(56)
    pooled = pool(pool_in, docs, pool_weight, pool_gain)
    ids = routes.reshape(-1)
    onehot = (ids[:, None] == jnp.arange(n_exp)[None, :]).astype(jnp.int32)
    rank = jnp.sum(onehot * (jnp.cumsum(onehot, axis=0) - 1), axis=1)
    place = (ids * cap + rank).reshape(length, TOPK)
    places = jnp.arange(slots)
    take = (place[:, 0][None, :] == places[:, None]) | (place[:, 1][None, :] == places[:, None])
    low = jnp.where(place[:, 0][:, None] == places[None, :], route_weights[:, 0][:, None], 0.0)
    mix = low + jnp.where(place[:, 1][:, None] == places[None, :], route_weights[:, 1][:, None], 0.0)
    mix_high, mix_low = split(mix)

    cuts_first = call(cut_first, [shape(1024, 256)] * 4, where, w_gate[0], w_up[0], flops=2**22)
    cuts_second = call(cut_second, [shape(512, 256)] * 4, where, w_down[0], flops=2**21)

    near = turns([pooled] * 4, GATHER)
    near = jnp.concatenate(near, axis=1)
    pooled_all = turns([near] * 4, SCATTER)
    updated = call(project, [shape(length, cols)], where, *pooled_all, out_weight, residual, flops=2**28)

    send = jnp.dot(take.astype(BF16), updated, preferred_element_type=F32).astype(BF16)
    arrived = lax.all_to_all(send.reshape(n_exp, cap, cols), SP, 0, 0, tiled=True).reshape(slots, cols)
    first = turns(cuts_first, SCATTER)
    second = turns(cuts_second, GATHER)
    made = experts(arrived, first, second, where, norm_gain.reshape(16, 256))
    back = lax.all_to_all(made.reshape(n_exp, cap, cols), SP, 0, 0, tiled=True).reshape(slots, cols)
    summed = jnp.dot(mix_high, back, preferred_element_type=F32) + jnp.dot(
        mix_low, back, preferred_element_type=F32
    )
    return (updated.astype(F32) + summed).astype(BF16)


def solution(mesh):
    torus = Mesh(mesh.devices.reshape(-1, 2, 4, 4), ("z", *PLANE))
    in_specs = (
        P(SP, TP),
        P(SP, TP),
        P(SP),
        P(TP, None, None),
        P(TP),
        P(None, TP),
        P(),
        P(SP, None),
        P(SP, None),
        P(SP, None, TP),
        P(SP, None, TP),
        P(SP, None, TP),
    )
    return jax.shard_map(layer, mesh=torus, in_specs=in_specs, out_specs=P(SP, TP), check_vma=False)
```

```python
import jax
import jax.numpy as jnp
import numpy as np
from jax import lax
from jax.experimental import pallas as pl
from jax.experimental.pallas import tpu as pltpu
from jax.sharding import Mesh
from jax.sharding import PartitionSpec as P


TOPK = 2
SP = ("z", "c")
TP = ("y", "x")
PLANE = ("c", "y", "x")
EPS = 1e-06
F32 = jnp.float32
BF16 = jnp.bfloat16
VMEM_BYTES = 20 * 2**20


RING = ((0, 0), (0, 1), (1, 1), (1, 0))


def blocks_of(shift):
    return [
        [(2 * v + shift + i) % 4 * 4 + (2 * h + shift + j) % 4 for i, j in RING]
        for v in (0, 1)
        for h in (0, 1)
    ]


GATHER = [blocks_of(0), blocks_of(1)]
SCATTER = [blocks_of(1), blocks_of(0)]


def both_cores(groups):
    return groups[0] + [[16 + m for m in group] for group in groups[1]]


def group_with(groups, member):
    return next(group for group in groups if member in group)


def tables():
    table = np.zeros((2, 16, 40), np.int32)
    for core in range(2):
        for me in range(16):
            gather, scatter = group_with(GATHER[core], me), group_with(SCATTER[core], me)
            p, q = scatter.index(me), gather.index(me)
            row = []
            for by in range(4):
                row += group_with(GATHER[core], scatter[(p + by) % 4])
            for by in range(4):
                row += group_with(SCATTER[core], gather[(q + by) % 4])
            table[core, me, :39] = row + gather + [p, q, 2 ** (1 + me % 4)]
    return table


FEATURES, HIDDEN, GAINS, IN_SCATTER, IN_GATHER, SPAN, SP_INDEX = 0, 16, 32, 36, 37, 38, 39


def a2a(blocks, groups):
    return lax.all_to_all(blocks, PLANE, 0, 0, tiled=True, axis_index_groups=both_cores(groups))


def turns(cuts, groups):
    got = [cuts[0]]
    for by in range(1, 4):
        pairs = [(g[i], g[(i + by) % 4]) for g in both_cores(groups) for i in range(4)]
        got.append(lax.ppermute(cuts[by], PLANE, pairs))
    return got


def shape(*dims, dtype=BF16):
    return jax.ShapeDtypeStruct(dims, dtype)


def whole():
    return pl.BlockSpec(memory_space=pltpu.VMEM)


def scalars():
    return pl.BlockSpec(memory_space=pltpu.SMEM)


def call(kernel, outs, specs, *args, flops, scratch=(), grid=(), out_specs=None):
    single = len(outs) == 1
    moved = sum(a.size * a.dtype.itemsize for a in (*args, *outs))
    out_specs = out_specs or [whole()] * len(outs)
    return pl.pallas_call(
        kernel,
        grid=grid,
        out_shape=outs[0] if single else tuple(outs),
        in_specs=specs,
        out_specs=out_specs[0] if single else tuple(out_specs),
        scratch_shapes=list(scratch),
        compiler_params=pltpu.CompilerParams(vmem_limit_bytes=VMEM_BYTES),
        cost_estimate=pl.CostEstimate(flops=flops, bytes_accessed=moved, transcendentals=0),
    )(*args)


def cut_first(where, gate, up, *outs):
    for by in range(4):
        for i in range(4):
            block = where[FEATURES + 4 * by + i]
            src = pl.ds(pl.multiple_of(block * 256, 256), 256)
            outs[by][pl.ds(256 * i, 256), pl.ds(0, 128)] = gate[src, :]
            outs[by][pl.ds(256 * i, 256), pl.ds(128, 128)] = up[src, :]


def cut_second(where, down, *outs):
    for by in range(4):
        for i in range(4):
            block = where[HIDDEN + 4 * by + i]
            outs[by][pl.ds(128 * i, 128), :] = down[pl.ds(pl.multiple_of(block * 128, 128), 128), :]


def pool(where, own, before, docs, docs_before, weight, gain, out, extended):
    length, width = own.shape
    sp_index, span = where[SP_INDEX], where[SPAN]
    extended[pl.ds(0, 16), :] = before[pl.ds(length - 16, 16), :].astype(F32)
    extended[pl.ds(16, length), :] = own[...].astype(F32)
    now = docs[...].astype(F32)
    earlier = jnp.where(sp_index == 0, -1.0, docs_before[:, pl.ds(length - 128, 128)].astype(F32))
    line = jnp.broadcast_to(jnp.concatenate([earlier, now], axis=1), (8, length + 128))
    count = jnp.ones((8, length), F32)
    for offset in range(1, 16):
        count = count + (pltpu.roll(line, offset, 1)[:, 128:] == line[:, 128:]).astype(F32)
    eighth = jnp.full((8, width), 0.125, F32)
    count = lax.dot_general(count, eighth, (((0,), (0,)), ((), ())), preferred_element_type=F32)
    count = jnp.minimum(count, span.astype(F32))
    values = own[...].astype(F32)
    totals = values
    for offset in range(1, 16):
        totals = totals + jnp.where(count > offset, extended[pl.ds(16 - offset, length), :], 0.0)
    diff = (totals / count - values).astype(BF16)
    mixed = jnp.dot(diff, weight[0], preferred_element_type=F32)
    pooled = (mixed * gain[...]).astype(BF16)
    for j in range(16):
        out[j] = pooled


def project(pooled, weight, residual, place, out, send):
    total = residual[...].astype(F32)
    for g in range(8):
        part = jnp.concatenate([pooled[2 * g], pooled[2 * g + 1]], axis=1)
        total = total + jnp.dot(part, weight[pl.ds(256 * g, 256), :], preferred_element_type=F32)
    updated = total.astype(BF16)
    out[...] = updated
    slots, length = send.shape[0], updated.shape[0]
    for i in range(slots // 256):
        slot = lax.broadcasted_iota(jnp.int32, (256, length), 0) + 256 * i
        take = ((place[pl.ds(0, 1), :] == slot) | (place[pl.ds(1, 1), :] == slot)).astype(F32).astype(BF16)
        send[pl.ds(256 * i, 256), :] = jnp.dot(take, updated, preferred_element_type=F32).astype(BF16)


def gate_up(where, got, gain, w0, w1, w2, w3, out, rows):
    ones = jnp.ones((8, 256), BF16)
    total = jnp.zeros((8, 256), F32)
    for g in range(4):
        value = got[g].astype(F32)
        rows[:, pl.ds(256 * g, 256)] = (value * gain[pl.ds(where[GAINS + g], 1), :]).astype(BF16)
        square = value * value
        high = square.astype(BF16)
        low = (square - high.astype(F32)).astype(BF16)
        for part in (high, low):
            total = total + lax.dot_general(ones, part, (((1,), (1,)), ((), ())), preferred_element_type=F32)
    line = lax.broadcasted_iota(jnp.int32, (8, 256), 0)
    high = total.astype(BF16).astype(F32)
    low = total - high
    extra = jnp.where(line == 0, high, jnp.where(line == 1, low, 0.0)).astype(BF16)
    for by, first in enumerate((w0, w1, w2, w3)):
        to = lax.rem(where[IN_SCATTER] + 4 - by, 4)
        out[to, 0, pl.ds(0, 256), :] = jnp.dot(rows[...], first[...], preferred_element_type=F32).astype(BF16)
        out[to, 0, pl.ds(256, 8), :] = extra


def activate(parts, out):
    extra = jnp.concatenate([parts[j, 0, pl.ds(256, 8), :].astype(F32) for j in range(4)], axis=0)
    ones = jnp.ones((32, 128), F32)
    total = lax.dot_general(extra, ones, (((0,), (0,)), ((), ())), preferred_element_type=F32)
    scale = lax.rsqrt(total / 4096 + EPS)
    tile = pl.ds(0, 256)
    gate = parts[0, 0, tile, pl.ds(0, 128)].astype(F32)
    up = parts[0, 0, tile, pl.ds(128, 128)].astype(F32)
    for j in range(1, 4):
        gate = gate + parts[j, 0, tile, pl.ds(0, 128)].astype(F32)
        up = up + parts[j, 0, tile, pl.ds(128, 128)].astype(F32)
    gate, up = gate * scale, up * scale
    act = (gate * jax.nn.sigmoid(gate) * up).astype(BF16)
    for j in range(4):
        out[j] = act


def down_rows(where, acts, w0, w1, w2, w3, out, rows):
    for h in range(4):
        rows[:, pl.ds(128 * h, 128)] = acts[h]
    for by, second in enumerate((w0, w1, w2, w3)):
        to = lax.rem(where[IN_GATHER] + 4 - by, 4)
        out[to] = jnp.dot(rows[...], second[...], preferred_element_type=F32).astype(BF16)


def experts(arrived, first, second, where, gain):
    count = arrived.shape[0]
    tiles = count // 256
    four = lambda width: pl.BlockSpec((4, 256, width), lambda i: (0, i, 0))
    padded = pl.BlockSpec((4, 1, 264, 256), lambda i: (0, i, 0, 0))
    got = a2a(jnp.broadcast_to(arrived[None], (4, *arrived.shape)), GATHER)
    part = call(
        gate_up,
        [shape(4, tiles, 264, 256)],
        [scalars(), four(256), whole(), *[whole()] * 4],
        where,
        got,
        gain,
        *first,
        flops=2**21 * count,
        scratch=[pltpu.VMEM((256, 1024), BF16)],
        grid=(tiles,),
        out_specs=[padded],
    )
    parts = a2a(part, SCATTER)
    act = call(
        activate, [shape(4, count, 128)], [padded], parts, flops=2**16 * count, grid=(tiles,), out_specs=[four(128)]
    )
    acts = a2a(act, SCATTER)
    part = call(
        down_rows,
        [shape(4, count, 256)],
        [scalars(), four(128), *[whole()] * 4],
        where,
        acts,
        *second,
        flops=2**20 * count,
        scratch=[pltpu.VMEM((256, 512), BF16)],
        grid=(tiles,),
        out_specs=[four(256)],
    )
    parts = a2a(part, GATHER)
    return jnp.sum(parts.astype(F32), axis=0).astype(BF16)


def split(value):
    high = lax.reduce_precision(value, 8, 7)
    return high.astype(BF16), (value - high).astype(BF16)


def layer(
    residual, pool_in, docs, pool_weight, pool_gain, out_weight, norm_gain, routes, route_weights, w_gate, w_up, w_down
):
    length, cols = residual.shape
    n_exp = lax.axis_size(SP)
    cap = length * TOPK * 3 // (2 * n_exp)
    slots = n_exp * cap
    where = lax.dynamic_slice(
        jnp.asarray(tables()), (lax.axis_index("c"), lax.axis_index(TP), 0), (1, 1, 40)
    ).reshape(40)
    where = where.at[SP_INDEX].set(lax.axis_index(SP))
    onward = [(i, i + 1) for i in range(n_exp - 1)]
    before = lax.ppermute(pool_in, SP, onward)
    docs_before = lax.ppermute(docs.reshape(1, length), SP, onward)
    pooled = call(
        pool,
        [shape(16, *pool_in.shape)],
        [scalars(), *[whole()] * 6],
        where,
        pool_in,
        before,
        docs.reshape(1, length),
        docs_before,
        pool_weight,
        pool_gain.reshape(1, -1),
        flops=2**23,
        scratch=[pltpu.VMEM((length + 16, pool_in.shape[1]), F32)],
    )
    ids = routes.reshape(-1)
    onehot = (ids[:, None] == jnp.arange(n_exp)[None, :]).astype(jnp.int32)
    rank = jnp.sum(onehot * (jnp.cumsum(onehot, axis=0) - 1), axis=1)
    place = (ids * cap + rank).reshape(length, TOPK)
    places = jnp.arange(slots)
    low = jnp.where(place[:, 0][:, None] == places[None, :], route_weights[:, 0][:, None], 0.0)
    mix = low + jnp.where(place[:, 1][:, None] == places[None, :], route_weights[:, 1][:, None], 0.0)
    mix_high, mix_low = split(mix)

    cuts_first = call(cut_first, [shape(1024, 256)] * 4, [scalars(), whole(), whole()], where, w_gate[0], w_up[0], flops=2**22)
    cuts_second = call(cut_second, [shape(512, 256)] * 4, [scalars(), whole()], where, w_down[0], flops=2**21)

    pooled_all = lax.all_to_all(pooled, TP, 0, 0, tiled=True)
    updated, send = call(
        project,
        [shape(length, cols), shape(slots, cols)],
        [whole()] * 4,
        pooled_all,
        out_weight,
        residual,
        place.T,
        flops=2**29,
    )
    arrived = lax.all_to_all(send.reshape(n_exp, cap, cols), SP, 0, 0, tiled=True).reshape(slots, cols)
    first = turns(cuts_first, SCATTER)
    second = turns(cuts_second, GATHER)
    made = experts(arrived, first, second, where, norm_gain.reshape(16, 256))
    back = lax.all_to_all(made.reshape(n_exp, cap, cols), SP, 0, 0, tiled=True).reshape(slots, cols)
    summed = jnp.dot(mix_high, back, preferred_element_type=F32) + jnp.dot(
        mix_low, back, preferred_element_type=F32
    )
    return (updated.astype(F32) + summed).astype(BF16)


def solution(mesh):
    torus = Mesh(mesh.devices.reshape(-1, 2, 4, 4), ("z", *PLANE))
    in_specs = (
        P(SP, TP),
        P(SP, TP),
        P(SP),
        P(TP, None, None),
        P(TP),
        P(None, TP),
        P(),
        P(SP, None),
        P(SP, None),
        P(SP, None, TP),
        P(SP, None, TP),
        P(SP, None, TP),
    )
    return jax.shard_map(layer, mesh=torus, in_specs=in_specs, out_specs=P(SP, TP), check_vma=False)
```

```python
import jax
import jax.numpy as jnp
import numpy as np
from jax import lax
from jax.experimental import pallas as pl
from jax.experimental.pallas import tpu as pltpu
from jax.sharding import Mesh
from jax.sharding import PartitionSpec as P


TOPK = 2
SP = ("z", "c")
TP = ("y", "x")
PLANE = ("c", "y", "x")
EPS = 1e-06
F32 = jnp.float32
BF16 = jnp.bfloat16
VMEM_BYTES = 20 * 2**20


def blocks_of(shift):
    return [
        [(2 * v + shift + i) % 4 * 4 + (2 * h + shift + j) % 4 for i in (0, 1) for j in (0, 1)]
        for v in (0, 1)
        for h in (0, 1)
    ]


GATHER = [blocks_of(1), blocks_of(0)]
SCATTER = [blocks_of(0), blocks_of(1)]


def both_cores(groups):
    return groups[0] + [[16 + m for m in group] for group in groups[1]]


def group_with(groups, member):
    return next(group for group in groups if member in group)


def tables():
    table = np.zeros((2, 16, 56), np.int32)
    for core in range(2):
        for me in range(16):
            gather, scatter = group_with(GATHER[core], me), group_with(SCATTER[core], me)
            p, q = scatter.index(me), gather.index(me)
            row = []
            for by in range(4):
                row += group_with(GATHER[core], scatter[(p + by) % 4])
            for by in range(4):
                row += group_with(SCATTER[core], gather[(q + by) % 4])
            channels = sum((group_with(GATHER[core], member) for member in scatter), [])
            table[core, me, :54] = row + gather + [p, q] + channels
    return table


FEATURES, HIDDEN, GAINS, IN_SCATTER, IN_GATHER, CHANNELS = 0, 16, 32, 36, 37, 38


def a2a(blocks, groups):
    return lax.all_to_all(blocks, PLANE, 0, 0, tiled=True, axis_index_groups=both_cores(groups))


def turns(cuts, groups):
    got = [cuts[0]]
    for by in range(1, 4):
        pairs = [(g[i], g[(i + by) % 4]) for g in both_cores(groups) for i in range(4)]
        got.append(lax.ppermute(cuts[by], PLANE, pairs))
    return got


def shape(*dims, dtype=BF16):
    return jax.ShapeDtypeStruct(dims, dtype)


def call(kernel, outs, *args, flops, scratch=()):
    single = len(outs) == 1
    moved = sum(a.size * a.dtype.itemsize for a in (*args, *outs))
    vmem = pl.BlockSpec(memory_space=pltpu.VMEM)
    return pl.pallas_call(
        kernel,
        out_shape=outs[0] if single else tuple(outs),
        in_specs=[pl.BlockSpec(memory_space=pltpu.SMEM) if a.dtype == jnp.int32 else vmem for a in args],
        out_specs=vmem if single else (vmem,) * len(outs),
        scratch_shapes=list(scratch),
        compiler_params=pltpu.CompilerParams(vmem_limit_bytes=VMEM_BYTES),
        cost_estimate=pl.CostEstimate(flops=flops, bytes_accessed=moved, transcendentals=0),
    )(*args)


def cut_first(where, gate, up, *outs):
    for by in range(4):
        for i in range(4):
            block = where[FEATURES + 4 * by + i]
            src = pl.ds(pl.multiple_of(block * 256, 256), 256)
            outs[by][pl.ds(256 * i, 256), pl.ds(0, 128)] = gate[src, :]
            outs[by][pl.ds(256 * i, 256), pl.ds(128, 128)] = up[src, :]


def cut_second(where, down, *outs):
    for by in range(4):
        for i in range(4):
            block = where[HIDDEN + 4 * by + i]
            outs[by][pl.ds(128 * i, 128), :] = down[pl.ds(pl.multiple_of(block * 128, 128), 128), :]


def project(where, pooled, weight, residual, out):
    total = residual[...].astype(F32)
    for j in range(4):
        rows = []
        for i in range(4):
            block = where[CHANNELS + 4 * j + i]
            rows.append(weight[pl.ds(pl.multiple_of(block * 128, 128), 128), :])
        part = jnp.concatenate([pooled[j, i] for i in range(4)], axis=1)
        total = total + jnp.dot(part, jnp.concatenate(rows, axis=0), preferred_element_type=F32)
    out[...] = total.astype(BF16)


def gate_up(where, got, gain, w0, w1, w2, w3, out, rows):
    count = got.shape[1]
    ones = jnp.ones((8, 256), BF16)
    tiles = count // 256
    for i in range(tiles):
        tile = pl.ds(256 * i, 256)
        total = jnp.zeros((8, 256), F32)
        for g in range(4):
            value = got[g, tile, :].astype(F32)
            rows[tile, pl.ds(256 * g, 256)] = (value * gain[pl.ds(where[GAINS + g], 1), :]).astype(BF16)
            square = value * value
            high = square.astype(BF16)
            low = (square - high.astype(F32)).astype(BF16)
            for part in (high, low):
                total = total + lax.dot_general(ones, part, (((1,), (1,)), ((), ())), preferred_element_type=F32)
        high = total.astype(BF16)
        low = (total - high.astype(F32)).astype(BF16)
        for j in range(4):
            out[j, pl.ds(count + 2 * i, 1), :] = high[:1]
            out[j, pl.ds(count + 2 * i + 1, 1), :] = low[:1]
    for by, first in enumerate((w0, w1, w2, w3)):
        to = lax.rem(where[IN_SCATTER] + 4 - by, 4)
        out[to, pl.ds(count + 2 * tiles, 8 - 2 * tiles), :] = jnp.zeros((8 - 2 * tiles, 256), BF16)
        for i in range(tiles):
            tile = pl.ds(256 * i, 256)
            out[to, tile, :] = jnp.dot(rows[tile, :], first[...], preferred_element_type=F32).astype(BF16)


def activate(parts, out):
    count = out.shape[1]
    extra = jnp.concatenate([parts[j, pl.ds(count, 8), :].astype(F32) for j in range(4)], axis=0)
    line = lax.broadcasted_iota(jnp.int32, (32, 128), 0) % 8
    for i in range(count // 256):
        tile = pl.ds(256 * i, 256)
        pick = ((line == 2 * i) | (line == 2 * i + 1)).astype(F32)
        total = lax.dot_general(extra, pick, (((0,), (0,)), ((), ())), preferred_element_type=F32)
        scale = lax.rsqrt(total / 4096 + EPS)
        gate = parts[0, tile, pl.ds(0, 128)].astype(F32)
        up = parts[0, tile, pl.ds(128, 128)].astype(F32)
        for j in range(1, 4):
            gate = gate + parts[j, tile, pl.ds(0, 128)].astype(F32)
            up = up + parts[j, tile, pl.ds(128, 128)].astype(F32)
        gate, up = gate * scale, up * scale
        act = (gate * jax.nn.sigmoid(gate) * up).astype(BF16)
        for j in range(4):
            out[j, tile, :] = act


def down_rows(where, acts, w0, w1, w2, w3, out, rows):
    count = acts.shape[1]
    for h in range(4):
        rows[:, pl.ds(128 * h, 128)] = acts[h]
    for by, second in enumerate((w0, w1, w2, w3)):
        to = lax.rem(where[IN_GATHER] + 4 - by, 4)
        for i in range(count // 256):
            tile = pl.ds(256 * i, 256)
            out[to, tile, :] = jnp.dot(rows[tile, :], second[...], preferred_element_type=F32).astype(BF16)


def experts(arrived, first, second, where, gain):
    count = arrived.shape[0]
    got = a2a(jnp.broadcast_to(arrived[None], (4, *arrived.shape)), GATHER)
    part = call(
        gate_up,
        [shape(4, count + 8, 256)],
        where,
        got,
        gain,
        *first,
        flops=2**21 * count,
        scratch=[pltpu.VMEM((count, 1024), BF16)],
    )
    parts = a2a(part, SCATTER)
    acts = a2a(call(activate, [shape(4, count, 128)], parts, flops=2**16 * count), SCATTER)
    part = call(
        down_rows,
        [shape(4, count, 256)],
        where,
        acts,
        *second,
        flops=2**20 * count,
        scratch=[pltpu.VMEM((count, 512), BF16)],
    )
    parts = a2a(part, GATHER)
    return jnp.sum(parts.astype(F32), axis=0).astype(BF16)


def pool(pool_in, docs, pool_weight, pool_gain):
    length, width = pool_in.shape
    sp_index = lax.axis_index(SP)
    group = lax.axis_index(TP)
    size = lax.axis_size(SP)
    reach = 15
    tail = docs[length - 16 :].astype(BF16)
    edge = jnp.concatenate([pool_in[length - reach :], jnp.pad(tail, (0, width - 16))[None]], axis=0)
    prev = lax.ppermute(edge, SP, [(i, i + 1) for i in range(size - 1)])
    extended = jnp.concatenate([prev[:reach], pool_in], axis=0).astype(F32)
    own_docs = docs.astype(F32)
    ext_docs = jnp.concatenate([prev[reach, 1:16].astype(F32), own_docs])
    places = sp_index * length + jnp.arange(length)
    span = 2 ** (1 + group % 4)
    totals = jnp.zeros((length, width), F32)
    counts = jnp.zeros((length,), F32)
    for offset in range(16):
        shifted = extended[reach - offset : reach - offset + length]
        prior = ext_docs[reach - offset : reach - offset + length]
        same = ((places >= offset) & (prior == own_docs) & (offset < span)).astype(F32)
        totals = totals + same[:, None] * shifted
        counts = counts + same
    diff = (totals / counts[:, None] - extended[reach:]).astype(BF16)
    mixed = jnp.dot(diff, pool_weight[0], preferred_element_type=F32)
    return (mixed * pool_gain).astype(BF16)


def split(value):
    high = lax.reduce_precision(value, 8, 7)
    return high.astype(BF16), (value - high).astype(BF16)


def layer(
    residual, pool_in, docs, pool_weight, pool_gain, out_weight, norm_gain, routes, route_weights, w_gate, w_up, w_down
):
    length, cols = residual.shape
    n_exp = lax.axis_size(SP)
    cap = length * TOPK * 3 // (2 * n_exp)
    slots = n_exp * cap
    where = lax.dynamic_slice(
        jnp.asarray(tables()), (lax.axis_index("c"), lax.axis_index(TP), 0), (1, 1, 56)
    ).reshape(56)
    pooled = pool(pool_in, docs, pool_weight, pool_gain)
    ids = routes.reshape(-1)
    onehot = (ids[:, None] == jnp.arange(n_exp)[None, :]).astype(jnp.int32)
    rank = jnp.sum(onehot * (jnp.cumsum(onehot, axis=0) - 1), axis=1)
    place = (ids * cap + rank).reshape(length, TOPK)
    places = jnp.arange(slots)
    take = (place[:, 0][None, :] == places[:, None]) | (place[:, 1][None, :] == places[:, None])
    low = jnp.where(place[:, 0][:, None] == places[None, :], route_weights[:, 0][:, None], 0.0)
    mix = low + jnp.where(place[:, 1][:, None] == places[None, :], route_weights[:, 1][:, None], 0.0)
    mix_high, mix_low = split(mix)

    cuts_first = call(cut_first, [shape(1024, 256)] * 4, where, w_gate[0], w_up[0], flops=2**22)
    cuts_second = call(cut_second, [shape(512, 256)] * 4, where, w_down[0], flops=2**21)

    near = a2a(jnp.broadcast_to(pooled[None], (4, *pooled.shape)), GATHER)
    pooled_all = a2a(jnp.broadcast_to(near[None], (4, *near.shape)), SCATTER)
    updated = call(project, [shape(length, cols)], where, pooled_all, out_weight, residual, flops=2**28)

    send = jnp.dot(take.astype(BF16), updated, preferred_element_type=F32).astype(BF16)
    arrived = lax.all_to_all(send.reshape(n_exp, cap, cols), SP, 0, 0, tiled=True).reshape(slots, cols)
    first = turns(cuts_first, SCATTER)
    second = turns(cuts_second, GATHER)
    made = experts(arrived, first, second, where, norm_gain.reshape(16, 256))
    back = lax.all_to_all(made.reshape(n_exp, cap, cols), SP, 0, 0, tiled=True).reshape(slots, cols)
    summed = jnp.dot(mix_high, back, preferred_element_type=F32) + jnp.dot(
        mix_low, back, preferred_element_type=F32
    )
    return (updated.astype(F32) + summed).astype(BF16)


def solution(mesh):
    torus = Mesh(mesh.devices.reshape(-1, 2, 4, 4), ("z", *PLANE))
    in_specs = (
        P(SP, TP),
        P(SP, TP),
        P(SP),
        P(TP, None, None),
        P(TP),
        P(None, TP),
        P(),
        P(SP, None),
        P(SP, None),
        P(SP, None, TP),
        P(SP, None, TP),
        P(SP, None, TP),
    )
    return jax.shard_map(layer, mesh=torus, in_specs=in_specs, out_specs=P(SP, TP), check_vma=False)
```

```python
import jax
import jax.numpy as jnp
import numpy as np
from jax import lax
from jax.experimental import pallas as pl
from jax.experimental.pallas import tpu as pltpu
from jax.sharding import Mesh
from jax.sharding import PartitionSpec as P


TOPK = 2
SP = ("z", "c")
TP = ("y", "x")
PLANE = ("c", "y", "x")
EPS = 1e-06
F32 = jnp.float32
BF16 = jnp.bfloat16
VMEM_BYTES = 20 * 2**20


def blocks_of(shift):
    return [
        [(2 * v + shift + i) % 4 * 4 + (2 * h + shift + j) % 4 for i in (0, 1) for j in (0, 1)]
        for v in (0, 1)
        for h in (0, 1)
    ]


GATHER = [blocks_of(1), blocks_of(0)]
SCATTER = [blocks_of(0), blocks_of(1)]


def both_cores(groups):
    return groups[0] + [[16 + m for m in group] for group in groups[1]]


def group_with(groups, member):
    return next(group for group in groups if member in group)


def tables():
    table = np.zeros((2, 16, 40), np.int32)
    for core in range(2):
        for me in range(16):
            gather, scatter = group_with(GATHER[core], me), group_with(SCATTER[core], me)
            p, q = scatter.index(me), gather.index(me)
            row = []
            for by in range(4):
                row += group_with(GATHER[core], scatter[(p + by) % 4])
            for by in range(4):
                row += group_with(SCATTER[core], gather[(q + by) % 4])
            table[core, me, :38] = row + gather + [p, q]
    return table


FEATURES, HIDDEN, GAINS, IN_SCATTER, IN_GATHER = 0, 16, 32, 36, 37


def a2a(blocks, groups):
    return lax.all_to_all(blocks, PLANE, 0, 0, tiled=True, axis_index_groups=both_cores(groups))


def turns(cuts, groups):
    got = [cuts[0]]
    for by in range(1, 4):
        pairs = [(g[i], g[(i + by) % 4]) for g in both_cores(groups) for i in range(4)]
        got.append(lax.ppermute(cuts[by], PLANE, pairs))
    return got


def shape(*dims, dtype=BF16):
    return jax.ShapeDtypeStruct(dims, dtype)


def call(kernel, outs, *args, flops, scratch=()):
    single = len(outs) == 1
    moved = sum(a.size * a.dtype.itemsize for a in (*args, *outs))
    vmem = pl.BlockSpec(memory_space=pltpu.VMEM)
    return pl.pallas_call(
        kernel,
        out_shape=outs[0] if single else tuple(outs),
        in_specs=[pl.BlockSpec(memory_space=pltpu.SMEM) if a.dtype == jnp.int32 else vmem for a in args],
        out_specs=vmem if single else (vmem,) * len(outs),
        scratch_shapes=list(scratch),
        compiler_params=pltpu.CompilerParams(vmem_limit_bytes=VMEM_BYTES),
        cost_estimate=pl.CostEstimate(flops=flops, bytes_accessed=moved, transcendentals=0),
    )(*args)


def cut_first(where, gate, up, *outs):
    for by in range(4):
        for i in range(4):
            block = where[FEATURES + 4 * by + i]
            src = pl.ds(pl.multiple_of(block * 256, 256), 256)
            outs[by][pl.ds(256 * i, 256), pl.ds(0, 128)] = gate[src, :]
            outs[by][pl.ds(256 * i, 256), pl.ds(128, 128)] = up[src, :]


def cut_second(where, down, *outs):
    for by in range(4):
        for i in range(4):
            block = where[HIDDEN + 4 * by + i]
            outs[by][pl.ds(128 * i, 128), :] = down[pl.ds(pl.multiple_of(block * 128, 128), 128), :]


def gate_up(where, got, gain, w0, w1, w2, w3, out, rows):
    count = got.shape[1]
    ones = jnp.ones((8, 256), BF16)
    tiles = count // 256
    for i in range(tiles):
        tile = pl.ds(256 * i, 256)
        total = jnp.zeros((8, 256), F32)
        for g in range(4):
            value = got[g, tile, :].astype(F32)
            rows[tile, pl.ds(256 * g, 256)] = (value * gain[pl.ds(where[GAINS + g], 1), :]).astype(BF16)
            square = value * value
            high = square.astype(BF16)
            low = (square - high.astype(F32)).astype(BF16)
            for part in (high, low):
                total = total + lax.dot_general(ones, part, (((1,), (1,)), ((), ())), preferred_element_type=F32)
        high = total.astype(BF16)
        low = (total - high.astype(F32)).astype(BF16)
        for j in range(4):
            out[j, pl.ds(count + 2 * i, 1), :] = high[:1]
            out[j, pl.ds(count + 2 * i + 1, 1), :] = low[:1]
    for by, first in enumerate((w0, w1, w2, w3)):
        to = lax.rem(where[IN_SCATTER] + 4 - by, 4)
        out[to, pl.ds(count + 2 * tiles, 8 - 2 * tiles), :] = jnp.zeros((8 - 2 * tiles, 256), BF16)
        for i in range(tiles):
            tile = pl.ds(256 * i, 256)
            out[to, tile, :] = jnp.dot(rows[tile, :], first[...], preferred_element_type=F32).astype(BF16)


def activate(parts, out):
    count = out.shape[1]
    extra = jnp.concatenate([parts[j, pl.ds(count, 8), :].astype(F32) for j in range(4)], axis=0)
    line = lax.broadcasted_iota(jnp.int32, (32, 128), 0) % 8
    for i in range(count // 256):
        tile = pl.ds(256 * i, 256)
        pick = ((line == 2 * i) | (line == 2 * i + 1)).astype(F32)
        total = lax.dot_general(extra, pick, (((0,), (0,)), ((), ())), preferred_element_type=F32)
        scale = lax.rsqrt(total / 4096 + EPS)
        gate = parts[0, tile, pl.ds(0, 128)].astype(F32)
        up = parts[0, tile, pl.ds(128, 128)].astype(F32)
        for j in range(1, 4):
            gate = gate + parts[j, tile, pl.ds(0, 128)].astype(F32)
            up = up + parts[j, tile, pl.ds(128, 128)].astype(F32)
        gate, up = gate * scale, up * scale
        act = (gate * jax.nn.sigmoid(gate) * up).astype(BF16)
        for j in range(4):
            out[j, tile, :] = act


def down_rows(where, acts, w0, w1, w2, w3, out, rows):
    count = acts.shape[1]
    for h in range(4):
        rows[:, pl.ds(128 * h, 128)] = acts[h]
    for by, second in enumerate((w0, w1, w2, w3)):
        to = lax.rem(where[IN_GATHER] + 4 - by, 4)
        for i in range(count // 256):
            tile = pl.ds(256 * i, 256)
            out[to, tile, :] = jnp.dot(rows[tile, :], second[...], preferred_element_type=F32).astype(BF16)


def experts(arrived, first, second, where, gain):
    count = arrived.shape[0]
    got = a2a(jnp.broadcast_to(arrived[None], (4, *arrived.shape)), GATHER)
    part = call(
        gate_up,
        [shape(4, count + 8, 256)],
        where,
        got,
        gain,
        *first,
        flops=2**21 * count,
        scratch=[pltpu.VMEM((count, 1024), BF16)],
    )
    parts = a2a(part, SCATTER)
    acts = a2a(call(activate, [shape(4, count, 128)], parts, flops=2**16 * count), SCATTER)
    part = call(
        down_rows,
        [shape(4, count, 256)],
        where,
        acts,
        *second,
        flops=2**20 * count,
        scratch=[pltpu.VMEM((count, 512), BF16)],
    )
    parts = a2a(part, GATHER)
    return jnp.sum(parts.astype(F32), axis=0).astype(BF16)


def pool(pool_in, docs, pool_weight, pool_gain):
    length, width = pool_in.shape
    sp_index = lax.axis_index(SP)
    group = lax.axis_index(TP)
    size = lax.axis_size(SP)
    reach = 15
    tail = docs[length - 16 :].astype(BF16)
    edge = jnp.concatenate([pool_in[length - reach :], jnp.pad(tail, (0, width - 16))[None]], axis=0)
    prev = lax.ppermute(edge, SP, [(i, i + 1) for i in range(size - 1)])
    extended = jnp.concatenate([prev[:reach], pool_in], axis=0).astype(F32)
    own_docs = docs.astype(F32)
    ext_docs = jnp.concatenate([prev[reach, 1:16].astype(F32), own_docs])
    places = sp_index * length + jnp.arange(length)
    span = 2 ** (1 + group % 4)
    totals = jnp.zeros((length, width), F32)
    counts = jnp.zeros((length,), F32)
    for offset in range(16):
        shifted = extended[reach - offset : reach - offset + length]
        prior = ext_docs[reach - offset : reach - offset + length]
        same = ((places >= offset) & (prior == own_docs) & (offset < span)).astype(F32)
        totals = totals + same[:, None] * shifted
        counts = counts + same
    diff = (totals / counts[:, None] - extended[reach:]).astype(BF16)
    mixed = jnp.dot(diff, pool_weight[0], preferred_element_type=F32)
    return (mixed * pool_gain).astype(BF16)


def split(value):
    high = lax.reduce_precision(value, 8, 7)
    return high.astype(BF16), (value - high).astype(BF16)


def layer(
    residual, pool_in, docs, pool_weight, pool_gain, out_weight, norm_gain, routes, route_weights, w_gate, w_up, w_down
):
    length, cols = residual.shape
    n_exp = lax.axis_size(SP)
    cap = length * TOPK * 3 // (2 * n_exp)
    slots = n_exp * cap
    where = lax.dynamic_slice(
        jnp.asarray(tables()), (lax.axis_index("c"), lax.axis_index(TP), 0), (1, 1, 40)
    ).reshape(40)
    pooled = pool(pool_in, docs, pool_weight, pool_gain)
    ids = routes.reshape(-1)
    onehot = (ids[:, None] == jnp.arange(n_exp)[None, :]).astype(jnp.int32)
    rank = jnp.sum(onehot * (jnp.cumsum(onehot, axis=0) - 1), axis=1)
    place = (ids * cap + rank).reshape(length, TOPK)
    places = jnp.arange(slots)
    take = (place[:, 0][None, :] == places[:, None]) | (place[:, 1][None, :] == places[:, None])
    low = jnp.where(place[:, 0][:, None] == places[None, :], route_weights[:, 0][:, None], 0.0)
    mix = low + jnp.where(place[:, 1][:, None] == places[None, :], route_weights[:, 1][:, None], 0.0)
    mix_high, mix_low = split(mix)

    cuts_first = call(cut_first, [shape(1024, 256)] * 4, where, w_gate[0], w_up[0], flops=2**22)
    cuts_second = call(cut_second, [shape(512, 256)] * 4, where, w_down[0], flops=2**21)

    pooled_all = lax.all_to_all(jnp.broadcast_to(pooled[None], (16, *pooled.shape)), TP, 0, 0, tiled=True)
    proj = jnp.einsum("gtc,gcd->td", pooled_all, out_weight.reshape(16, 128, cols), preferred_element_type=F32)
    updated = (residual.astype(F32) + proj).astype(BF16)

    send = jnp.dot(take.astype(BF16), updated, preferred_element_type=F32).astype(BF16)
    arrived = lax.all_to_all(send.reshape(n_exp, cap, cols), SP, 0, 0, tiled=True).reshape(slots, cols)
    first = turns(cuts_first, SCATTER)
    second = turns(cuts_second, GATHER)
    made = experts(arrived, first, second, where, norm_gain.reshape(16, 256))
    back = lax.all_to_all(made.reshape(n_exp, cap, cols), SP, 0, 0, tiled=True).reshape(slots, cols)
    summed = jnp.dot(mix_high, back, preferred_element_type=F32) + jnp.dot(
        mix_low, back, preferred_element_type=F32
    )
    return (updated.astype(F32) + summed).astype(BF16)


def solution(mesh):
    torus = Mesh(mesh.devices.reshape(-1, 2, 4, 4), ("z", *PLANE))
    in_specs = (
        P(SP, TP),
        P(SP, TP),
        P(SP),
        P(TP, None, None),
        P(TP),
        P(None, TP),
        P(),
        P(SP, None),
        P(SP, None),
        P(SP, None, TP),
        P(SP, None, TP),
        P(SP, None, TP),
    )
    return jax.shard_map(layer, mesh=torus, in_specs=in_specs, out_specs=P(SP, TP), check_vma=False)
```

```python
import jax
import jax.numpy as jnp
import numpy as np
from jax import lax
from jax.experimental import pallas as pl
from jax.experimental.pallas import tpu as pltpu
from jax.sharding import Mesh
from jax.sharding import PartitionSpec as P


TOPK = 2
SP = ("z", "c")
TP = ("y", "x")
PLANE = ("c", "y", "x")
EPS = 1e-06
F32 = jnp.float32
BF16 = jnp.bfloat16
VMEM_BYTES = 20 * 2**20
LARGE = 58 * 2**20


def blocks_of(shift):
    return [
        [(2 * v + shift + i) % 4 * 4 + (2 * h + shift + j) % 4 for i in (0, 1) for j in (0, 1)]
        for v in (0, 1)
        for h in (0, 1)
    ]


GATHER = [blocks_of(1), blocks_of(0)]
SCATTER = [blocks_of(0), blocks_of(1)]


def both_cores(groups):
    return groups[0] + [[16 + m for m in group] for group in groups[1]]


def group_with(groups, member):
    return next(group for group in groups if member in group)


def tables():
    table = np.zeros((2, 16, 40), np.int32)
    for core in range(2):
        for me in range(16):
            gather, scatter = group_with(GATHER[core], me), group_with(SCATTER[core], me)
            p, q = scatter.index(me), gather.index(me)
            row = []
            for by in range(4):
                row += group_with(GATHER[core], scatter[(p + by) % 4])
            for by in range(4):
                row += group_with(SCATTER[core], gather[(q + by) % 4])
            table[core, me, :39] = row + gather + [p, q, 2 ** (1 + me % 4)]
    return table


FEATURES, HIDDEN, GAINS, IN_SCATTER, IN_GATHER, SPAN, SP_INDEX = 0, 16, 32, 36, 37, 38, 39


def a2a(blocks, groups):
    return lax.all_to_all(blocks, PLANE, 0, 0, tiled=True, axis_index_groups=both_cores(groups))


def turns(cuts, groups):
    got = [cuts[0]]
    for by in range(1, 4):
        pairs = [(g[i], g[(i + by) % 4]) for g in both_cores(groups) for i in range(4)]
        got.append(lax.ppermute(cuts[by], PLANE, pairs))
    return got


def shape(*dims, dtype=BF16):
    return jax.ShapeDtypeStruct(dims, dtype)


def call(kernel, outs, *args, flops, scratch=(), vmem=VMEM_BYTES, tables=1, fetched=0):
    single = len(outs) == 1
    moved = sum(a.size * a.dtype.itemsize for a in (*args, *outs))
    whole = pl.BlockSpec(memory_space=pltpu.VMEM)
    specs = [pl.BlockSpec(memory_space=pltpu.SMEM)] * tables
    specs += [whole] * (len(args) - tables - fetched) + [pl.BlockSpec(memory_space=pltpu.HBM)] * fetched
    return pl.pallas_call(
        kernel,
        out_shape=outs[0] if single else tuple(outs),
        in_specs=specs,
        out_specs=whole if single else (whole,) * len(outs),
        scratch_shapes=list(scratch),
        compiler_params=pltpu.CompilerParams(vmem_limit_bytes=vmem),
        cost_estimate=pl.CostEstimate(flops=flops, bytes_accessed=moved, transcendentals=0),
    )(*args)


def cut_first(where, gate, up, *outs):
    for by in range(4):
        for i in range(4):
            block = where[FEATURES + 4 * by + i]
            src = pl.ds(pl.multiple_of(block * 256, 256), 256)
            outs[by][pl.ds(256 * i, 256), pl.ds(0, 128)] = gate[src, :]
            outs[by][pl.ds(256 * i, 256), pl.ds(128, 128)] = up[src, :]


def cut_second(where, down, *outs):
    for by in range(4):
        for i in range(4):
            block = where[HIDDEN + 4 * by + i]
            outs[by][pl.ds(128 * i, 128), :] = down[pl.ds(pl.multiple_of(block * 128, 128), 128), :]


def fetches(sources, held, arrived):
    return [pltpu.make_async_copy(w, held.at[by], arrived.at[by]) for by, w in enumerate(sources)]


def gate_up(where, got, gain, w0, w1, w2, w3, out, rows, held, arrived):
    copies = fetches((w0, w1, w2, w3), held, arrived)
    for copy in copies:
        copy.start()
    count = got.shape[1]
    ones = jnp.ones((8, 256), BF16)
    tiles = count // 256
    for i in range(tiles):
        tile = pl.ds(256 * i, 256)
        total = jnp.zeros((8, 256), F32)
        for g in range(4):
            value = got[g, tile, :].astype(F32)
            rows[tile, pl.ds(256 * g, 256)] = (value * gain[pl.ds(where[GAINS + g], 1), :]).astype(BF16)
            square = value * value
            high = square.astype(BF16)
            low = (square - high.astype(F32)).astype(BF16)
            for part in (high, low):
                total = total + lax.dot_general(ones, part, (((1,), (1,)), ((), ())), preferred_element_type=F32)
        high = total.astype(BF16)
        low = (total - high.astype(F32)).astype(BF16)
        for j in range(4):
            out[j, pl.ds(count + 2 * i, 1), :] = high[:1]
            out[j, pl.ds(count + 2 * i + 1, 1), :] = low[:1]
    for by, copy in enumerate(copies):
        copy.wait()
        to = lax.rem(where[IN_SCATTER] + 4 - by, 4)
        out[to, pl.ds(count + 2 * tiles, 8 - 2 * tiles), :] = jnp.zeros((8 - 2 * tiles, 256), BF16)
        for i in range(tiles):
            tile = pl.ds(256 * i, 256)
            out[to, tile, :] = jnp.dot(rows[tile, :], held[by], preferred_element_type=F32).astype(BF16)


def activate(parts, out):
    count = out.shape[1]
    extra = jnp.concatenate([parts[j, pl.ds(count, 8), :].astype(F32) for j in range(4)], axis=0)
    line = lax.broadcasted_iota(jnp.int32, (32, 128), 0) % 8
    for i in range(count // 256):
        tile = pl.ds(256 * i, 256)
        pick = ((line == 2 * i) | (line == 2 * i + 1)).astype(F32)
        total = lax.dot_general(extra, pick, (((0,), (0,)), ((), ())), preferred_element_type=F32)
        scale = lax.rsqrt(total / 4096 + EPS)
        gate = parts[0, tile, pl.ds(0, 128)].astype(F32)
        up = parts[0, tile, pl.ds(128, 128)].astype(F32)
        for j in range(1, 4):
            gate = gate + parts[j, tile, pl.ds(0, 128)].astype(F32)
            up = up + parts[j, tile, pl.ds(128, 128)].astype(F32)
        gate, up = gate * scale, up * scale
        act = (gate * jax.nn.sigmoid(gate) * up).astype(BF16)
        for j in range(4):
            out[j, tile, :] = act


def down_rows(where, acts, w0, w1, w2, w3, out, rows, held, arrived):
    copies = fetches((w0, w1, w2, w3), held, arrived)
    for copy in copies:
        copy.start()
    count = acts.shape[1]
    for h in range(4):
        rows[:, pl.ds(128 * h, 128)] = acts[h]
    for by, copy in enumerate(copies):
        copy.wait()
        to = lax.rem(where[IN_GATHER] + 4 - by, 4)
        for i in range(count // 256):
            tile = pl.ds(256 * i, 256)
            out[to, tile, :] = jnp.dot(rows[tile, :], held[by], preferred_element_type=F32).astype(BF16)


def experts(arrived, first, second, where, gain):
    count = arrived.shape[0]
    got = a2a(jnp.broadcast_to(arrived[None], (4, *arrived.shape)), GATHER)
    part = call(
        gate_up,
        [shape(4, count + 8, 256)],
        where,
        got,
        gain,
        *first,
        flops=2**21 * count,
        scratch=[pltpu.VMEM((count, 1024), BF16), pltpu.VMEM((4, 1024, 256), BF16), pltpu.SemaphoreType.DMA((4,))],
        fetched=4,
    )
    parts = a2a(part, SCATTER)
    acts = a2a(call(activate, [shape(4, count, 128)], parts, flops=2**16 * count, tables=0), SCATTER)
    part = call(
        down_rows,
        [shape(4, count, 256)],
        where,
        acts,
        *second,
        flops=2**20 * count,
        scratch=[pltpu.VMEM((count, 512), BF16), pltpu.VMEM((4, 512, 256), BF16), pltpu.SemaphoreType.DMA((4,))],
        fetched=4,
    )
    parts = a2a(part, GATHER)
    return jnp.sum(parts.astype(F32), axis=0).astype(BF16)


def pool(where, own, before, docs, docs_before, weight, gain, out, extended):
    length, width = own.shape
    sp_index, span = where[SP_INDEX], where[SPAN]
    extended[pl.ds(0, 16), :] = before[pl.ds(length - 16, 16), :].astype(F32)
    extended[pl.ds(16, length), :] = own[...].astype(F32)
    now = docs[...].astype(F32)
    earlier = jnp.where(sp_index == 0, -1.0, docs_before[:, pl.ds(length - 128, 128)].astype(F32))
    line = jnp.broadcast_to(jnp.concatenate([earlier, now], axis=1), (8, length + 128))
    count = jnp.ones((8, length), F32)
    for offset in range(1, 16):
        count = count + (pltpu.roll(line, offset, 1)[:, 128:] == line[:, 128:]).astype(F32)
    eighth = jnp.full((8, width), 0.125, F32)
    count = lax.dot_general(count, eighth, (((0,), (0,)), ((), ())), preferred_element_type=F32)
    count = jnp.minimum(count, span.astype(F32))
    values = own[...].astype(F32)
    totals = values
    for offset in range(1, 16):
        totals = totals + jnp.where(count > offset, extended[pl.ds(16 - offset, length), :], 0.0)
    diff = (totals / count - values).astype(BF16)
    mixed = jnp.dot(diff, weight[0], preferred_element_type=F32)
    pooled = (mixed * gain[...]).astype(BF16)
    for j in range(16):
        out[j] = pooled


def split(value):
    high = lax.reduce_precision(value, 8, 7)
    return high.astype(BF16), (value - high).astype(BF16)


def layer(
    residual, pool_in, docs, pool_weight, pool_gain, out_weight, norm_gain, routes, route_weights, w_gate, w_up, w_down
):
    length, cols = residual.shape
    n_exp = lax.axis_size(SP)
    cap = length * TOPK * 3 // (2 * n_exp)
    slots = n_exp * cap
    where = lax.dynamic_slice(
        jnp.asarray(tables()), (lax.axis_index("c"), lax.axis_index(TP), 0), (1, 1, 40)
    ).reshape(40)
    where = where.at[SP_INDEX].set(lax.axis_index(SP))
    onward = [(i, i + 1) for i in range(n_exp - 1)]
    before = lax.ppermute(pool_in, SP, onward)
    docs_before = lax.ppermute(docs.reshape(1, length), SP, onward)
    pooled = call(
        pool,
        [shape(16, *pool_in.shape)],
        where,
        pool_in,
        before,
        docs.reshape(1, length),
        docs_before,
        pool_weight,
        pool_gain.reshape(1, -1),
        flops=2**23,
        scratch=[pltpu.VMEM((length + 16, pool_in.shape[1]), F32)],
        vmem=LARGE,
    )
    ids = routes.reshape(-1)
    onehot = (ids[:, None] == jnp.arange(n_exp)[None, :]).astype(jnp.int32)
    rank = jnp.sum(onehot * (jnp.cumsum(onehot, axis=0) - 1), axis=1)
    place = (ids * cap + rank).reshape(length, TOPK)
    places = jnp.arange(slots)
    take = (place[:, 0][None, :] == places[:, None]) | (place[:, 1][None, :] == places[:, None])
    low = jnp.where(place[:, 0][:, None] == places[None, :], route_weights[:, 0][:, None], 0.0)
    mix = low + jnp.where(place[:, 1][:, None] == places[None, :], route_weights[:, 1][:, None], 0.0)
    mix_high, mix_low = split(mix)

    cuts_first = call(cut_first, [shape(1024, 256)] * 4, where, w_gate[0], w_up[0], flops=2**22, vmem=LARGE)
    cuts_second = call(cut_second, [shape(512, 256)] * 4, where, w_down[0], flops=2**21, vmem=LARGE)

    pooled_all = lax.all_to_all(pooled, TP, 0, 0, tiled=True)
    proj = jnp.einsum("gtc,gcd->td", pooled_all, out_weight.reshape(16, 128, cols), preferred_element_type=F32)
    updated = (residual.astype(F32) + proj).astype(BF16)

    send = jnp.dot(take.astype(BF16), updated, preferred_element_type=F32).astype(BF16)
    arrived = lax.all_to_all(send.reshape(n_exp, cap, cols), SP, 0, 0, tiled=True).reshape(slots, cols)
    first = turns(cuts_first, SCATTER)
    second = turns(cuts_second, GATHER)
    made = experts(arrived, first, second, where, norm_gain.reshape(16, 256))
    back = lax.all_to_all(made.reshape(n_exp, cap, cols), SP, 0, 0, tiled=True).reshape(slots, cols)
    summed = jnp.dot(mix_high, back, preferred_element_type=F32) + jnp.dot(
        mix_low, back, preferred_element_type=F32
    )
    return (updated.astype(F32) + summed).astype(BF16)


def solution(mesh):
    torus = Mesh(mesh.devices.reshape(-1, 2, 4, 4), ("z", *PLANE))
    in_specs = (
        P(SP, TP),
        P(SP, TP),
        P(SP),
        P(TP, None, None),
        P(TP),
        P(None, TP),
        P(),
        P(SP, None),
        P(SP, None),
        P(SP, None, TP),
        P(SP, None, TP),
        P(SP, None, TP),
    )
    return jax.shard_map(layer, mesh=torus, in_specs=in_specs, out_specs=P(SP, TP), check_vma=False)
```

```python
import jax
import jax.numpy as jnp
import numpy as np
from jax import lax
from jax.experimental import pallas as pl
from jax.experimental.pallas import tpu as pltpu
from jax.sharding import Mesh
from jax.sharding import PartitionSpec as P


TOPK = 2
SP = ("z", "c")
TP = ("y", "x")
PLANE = ("c", "y", "x")
EPS = 1e-06
F32 = jnp.float32
BF16 = jnp.bfloat16
VMEM_BYTES = 20 * 2**20
LARGE = 58 * 2**20


def blocks_of(shift):
    return [
        [(2 * v + shift + i) % 4 * 4 + (2 * h + shift + j) % 4 for i in (0, 1) for j in (0, 1)]
        for v in (0, 1)
        for h in (0, 1)
    ]


GATHER = [blocks_of(1), blocks_of(0)]
SCATTER = [blocks_of(0), blocks_of(1)]


HALVES = [
    [[y * 4 + x for y in (v, v + 1) for x in range(4)] for v in (0, 2)],
    [[y * 4 + x for y in range(4) for x in (h, h + 1)] for h in (0, 2)],
]


def partner(core, member):
    y, x = divmod(member, 4)
    return (3 - y) * 4 + x if core == 0 else y * 4 + 3 - x


PARTNERS = [(16 * core + m, 16 * core + partner(core, m)) for core in range(2) for m in range(16)]


def both_cores(groups):
    return groups[0] + [[16 + m for m in group] for group in groups[1]]


def group_with(groups, member):
    return next(group for group in groups if member in group)


def tables():
    table = np.zeros((2, 16, 56), np.int32)
    for core in range(2):
        for me in range(16):
            gather, scatter = group_with(GATHER[core], me), group_with(SCATTER[core], me)
            p, q = scatter.index(me), gather.index(me)
            row = []
            for by in range(4):
                row += group_with(GATHER[core], scatter[(p + by) % 4])
            for by in range(4):
                row += group_with(SCATTER[core], gather[(q + by) % 4])
            halves = group_with(HALVES[core], me) + group_with(HALVES[core], partner(core, me))
            table[core, me, :39] = row + gather + [p, q, 2 ** (1 + me % 4)]
            table[core, me, 40:] = halves
    return table


FEATURES, HIDDEN, GAINS, IN_SCATTER, IN_GATHER, SPAN, SP_INDEX, CHANNELS, OTHERS = 0, 16, 32, 36, 37, 38, 39, 40, 48


def a2a(blocks, groups):
    return lax.all_to_all(blocks, PLANE, 0, 0, tiled=True, axis_index_groups=both_cores(groups))


def turns(cuts, groups):
    got = []
    for by in range(1, 4):
        pairs = [(g[i], g[(i + by) % 4]) for g in both_cores(groups) for i in range(4)]
        got.append(lax.ppermute(cuts[by - 1], PLANE, pairs))
    return got


def shape(*dims, dtype=BF16):
    return jax.ShapeDtypeStruct(dims, dtype)


def call(kernel, outs, *args, flops, scratch=(), vmem=VMEM_BYTES, tables=1, fetched=0):
    single = len(outs) == 1
    moved = sum(a.size * a.dtype.itemsize for a in (*args, *outs))
    whole = pl.BlockSpec(memory_space=pltpu.VMEM)
    specs = [pl.BlockSpec(memory_space=pltpu.SMEM)] * tables
    specs += [whole] * (len(args) - tables - fetched) + [pl.BlockSpec(memory_space=pltpu.HBM)] * fetched
    return pl.pallas_call(
        kernel,
        out_shape=outs[0] if single else tuple(outs),
        in_specs=specs,
        out_specs=whole if single else (whole,) * len(outs),
        scratch_shapes=list(scratch),
        compiler_params=pltpu.CompilerParams(vmem_limit_bytes=vmem),
        cost_estimate=pl.CostEstimate(flops=flops, bytes_accessed=moved, transcendentals=0),
    )(*args)


def cut_out(where, weight, out):
    for i in range(8):
        src = pl.ds(pl.multiple_of(where[OTHERS + i] * 128, 128), 128)
        out[pl.ds(128 * i, 128), :] = weight[src, :]


def cut_first(where, gate, up, *outs):
    for by in range(1, 4):
        for i in range(4):
            block = where[FEATURES + 4 * by + i]
            src = pl.ds(pl.multiple_of(block * 256, 256), 256)
            outs[by - 1][pl.ds(256 * i, 256), pl.ds(0, 128)] = gate[src, :]
            outs[by - 1][pl.ds(256 * i, 256), pl.ds(128, 128)] = up[src, :]


def cut_second(where, down, *outs):
    for by in range(1, 4):
        for i in range(4):
            block = where[HIDDEN + 4 * by + i]
            outs[by - 1][pl.ds(128 * i, 128), :] = down[pl.ds(pl.multiple_of(block * 128, 128), 128), :]


def project(where, pooled, weight, theirs, residual, mine_out, theirs_out):
    rows = [weight[pl.ds(pl.multiple_of(where[CHANNELS + i] * 128, 128), 128), :] for i in range(8)]
    total = residual[...].astype(F32)
    other = jnp.zeros(total.shape, F32)
    for i in range(4):
        part = jnp.concatenate([pooled[2 * i], pooled[2 * i + 1]], axis=1)
        total = total + jnp.dot(part, jnp.concatenate(rows[2 * i : 2 * i + 2], axis=0), preferred_element_type=F32)
        other = other + jnp.dot(part, theirs[pl.ds(256 * i, 256), :], preferred_element_type=F32)
    mine_out[...] = total
    theirs_out[...] = other.astype(BF16)


def finish(mine, received, place, out, send):
    updated = (mine[...] + received[...].astype(F32)).astype(BF16)
    out[...] = updated
    slots, length = send.shape[0], updated.shape[0]
    for i in range(slots // 256):
        slot = lax.broadcasted_iota(jnp.int32, (256, length), 0) + 256 * i
        take = ((place[pl.ds(0, 1), :] == slot) | (place[pl.ds(1, 1), :] == slot)).astype(F32).astype(BF16)
        send[pl.ds(256 * i, 256), :] = jnp.dot(take, updated, preferred_element_type=F32).astype(BF16)


def fetches(sources, held, arrived):
    return [pltpu.make_async_copy(w, held.at[by + 1], arrived.at[by]) for by, w in enumerate(sources)]


def gate_up(where, got, gain, gate, up, w1, w2, w3, out, rows, held, arrived):
    copies = fetches((w1, w2, w3), held, arrived)
    for i in range(4):
        src = pl.ds(pl.multiple_of(where[FEATURES + i] * 256, 256), 256)
        to = held.at[0, pl.ds(256 * i, 256)]
        copies.append(pltpu.make_async_copy(gate.at[src], to.at[:, pl.ds(0, 128)], arrived.at[3 + 2 * i]))
        copies.append(pltpu.make_async_copy(up.at[src], to.at[:, pl.ds(128, 128)], arrived.at[4 + 2 * i]))
    for copy in copies:
        copy.start()
    count = got.shape[1]
    ones = jnp.ones((8, 256), BF16)
    tiles = count // 256
    for i in range(tiles):
        tile = pl.ds(256 * i, 256)
        total = jnp.zeros((8, 256), F32)
        for g in range(4):
            value = got[g, tile, :].astype(F32)
            rows[tile, pl.ds(256 * g, 256)] = (value * gain[pl.ds(where[GAINS + g], 1), :]).astype(BF16)
            square = value * value
            high = square.astype(BF16)
            low = (square - high.astype(F32)).astype(BF16)
            for part in (high, low):
                total = total + lax.dot_general(ones, part, (((1,), (1,)), ((), ())), preferred_element_type=F32)
        high = total.astype(BF16)
        low = (total - high.astype(F32)).astype(BF16)
        for j in range(4):
            out[j, pl.ds(count + 2 * i, 1), :] = high[:1]
            out[j, pl.ds(count + 2 * i + 1, 1), :] = low[:1]
    for by in range(4):
        for copy in copies[3:] if by == 0 else copies[by - 1 : by]:
            copy.wait()
        to = lax.rem(where[IN_SCATTER] + 4 - by, 4)
        out[to, pl.ds(count + 2 * tiles, 8 - 2 * tiles), :] = jnp.zeros((8 - 2 * tiles, 256), BF16)
        for i in range(tiles):
            tile = pl.ds(256 * i, 256)
            out[to, tile, :] = jnp.dot(rows[tile, :], held[by], preferred_element_type=F32).astype(BF16)


def activate(parts, out):
    count = out.shape[1]
    extra = jnp.concatenate([parts[j, pl.ds(count, 8), :].astype(F32) for j in range(4)], axis=0)
    line = lax.broadcasted_iota(jnp.int32, (32, 128), 0) % 8
    for i in range(count // 256):
        tile = pl.ds(256 * i, 256)
        pick = ((line == 2 * i) | (line == 2 * i + 1)).astype(F32)
        total = lax.dot_general(extra, pick, (((0,), (0,)), ((), ())), preferred_element_type=F32)
        scale = lax.rsqrt(total / 4096 + EPS)
        gate = parts[0, tile, pl.ds(0, 128)].astype(F32)
        up = parts[0, tile, pl.ds(128, 128)].astype(F32)
        for j in range(1, 4):
            gate = gate + parts[j, tile, pl.ds(0, 128)].astype(F32)
            up = up + parts[j, tile, pl.ds(128, 128)].astype(F32)
        gate, up = gate * scale, up * scale
        act = (gate * jax.nn.sigmoid(gate) * up).astype(BF16)
        for j in range(4):
            out[j, tile, :] = act


def down_rows(where, acts, down, w1, w2, w3, out, rows, held, arrived):
    copies = fetches((w1, w2, w3), held, arrived)
    for i in range(4):
        src = pl.ds(pl.multiple_of(where[HIDDEN + i] * 128, 128), 128)
        copies.append(pltpu.make_async_copy(down.at[src], held.at[0, pl.ds(128 * i, 128)], arrived.at[3 + i]))
    for copy in copies:
        copy.start()
    count = acts.shape[1]
    for h in range(4):
        rows[:, pl.ds(128 * h, 128)] = acts[h]
    for by in range(4):
        for copy in copies[3:] if by == 0 else copies[by - 1 : by]:
            copy.wait()
        to = lax.rem(where[IN_GATHER] + 4 - by, 4)
        for i in range(count // 256):
            tile = pl.ds(256 * i, 256)
            out[to, tile, :] = jnp.dot(rows[tile, :], held[by], preferred_element_type=F32).astype(BF16)


def experts(arrived, first, second, where, gain):
    count = arrived.shape[0]
    got = a2a(jnp.broadcast_to(arrived[None], (4, *arrived.shape)), GATHER)
    part = call(
        gate_up,
        [shape(4, count + 8, 256)],
        where,
        got,
        gain,
        *first,
        flops=2**21 * count,
        scratch=[pltpu.VMEM((count, 1024), BF16), pltpu.VMEM((4, 1024, 256), BF16), pltpu.SemaphoreType.DMA((11,))],
        fetched=5,
    )
    parts = a2a(part, SCATTER)
    acts = a2a(call(activate, [shape(4, count, 128)], parts, flops=2**16 * count, tables=0), SCATTER)
    part = call(
        down_rows,
        [shape(4, count, 256)],
        where,
        acts,
        *second,
        flops=2**20 * count,
        scratch=[pltpu.VMEM((count, 512), BF16), pltpu.VMEM((4, 512, 256), BF16), pltpu.SemaphoreType.DMA((7,))],
        fetched=4,
    )
    parts = a2a(part, GATHER)
    return jnp.sum(parts.astype(F32), axis=0).astype(BF16)


def pool(where, own, before, docs, docs_before, weight, gain, out, extended):
    length, width = own.shape
    sp_index, span = where[SP_INDEX], where[SPAN]
    extended[pl.ds(0, 16), :] = before[pl.ds(length - 16, 16), :].astype(F32)
    extended[pl.ds(16, length), :] = own[...].astype(F32)
    now = docs[...].astype(F32)
    earlier = jnp.where(sp_index == 0, -1.0, docs_before[:, pl.ds(length - 128, 128)].astype(F32))
    line = jnp.broadcast_to(jnp.concatenate([earlier, now], axis=1), (8, length + 128))
    count = jnp.ones((8, length), F32)
    for offset in range(1, 16):
        count = count + (pltpu.roll(line, offset, 1)[:, 128:] == line[:, 128:]).astype(F32)
    eighth = jnp.full((8, width), 0.125, F32)
    count = lax.dot_general(count, eighth, (((0,), (0,)), ((), ())), preferred_element_type=F32)
    count = jnp.minimum(count, span.astype(F32))
    values = own[...].astype(F32)
    totals = values
    for offset in range(1, 16):
        totals = totals + jnp.where(count > offset, extended[pl.ds(16 - offset, length), :], 0.0)
    diff = (totals / count - values).astype(BF16)
    mixed = jnp.dot(diff, weight[0], preferred_element_type=F32)
    pooled = (mixed * gain[...]).astype(BF16)
    for j in range(8):
        out[j] = pooled


def split(value):
    high = lax.reduce_precision(value, 8, 7)
    return high.astype(BF16), (value - high).astype(BF16)


def layer(
    residual, pool_in, docs, pool_weight, pool_gain, out_weight, norm_gain, routes, route_weights, w_gate, w_up, w_down
):
    length, cols = residual.shape
    n_exp = lax.axis_size(SP)
    cap = length * TOPK * 3 // (2 * n_exp)
    slots = n_exp * cap
    where = lax.dynamic_slice(
        jnp.asarray(tables()), (lax.axis_index("c"), lax.axis_index(TP), 0), (1, 1, 56)
    ).reshape(56)
    where = where.at[SP_INDEX].set(lax.axis_index(SP))
    onward = [(i, i + 1) for i in range(n_exp - 1)]
    before = lax.ppermute(pool_in, SP, onward)
    docs_before = lax.ppermute(docs.reshape(1, length), SP, onward)
    pooled = call(
        pool,
        [shape(8, *pool_in.shape)],
        where,
        pool_in,
        before,
        docs.reshape(1, length),
        docs_before,
        pool_weight,
        pool_gain.reshape(1, -1),
        flops=2**23,
        scratch=[pltpu.VMEM((length + 16, pool_in.shape[1]), F32)],
        vmem=LARGE,
    )
    ids = routes.reshape(-1)
    onehot = (ids[:, None] == jnp.arange(n_exp)[None, :]).astype(jnp.int32)
    rank = jnp.sum(onehot * (jnp.cumsum(onehot, axis=0) - 1), axis=1)
    place = (ids * cap + rank).reshape(length, TOPK)
    places = jnp.arange(slots)
    low = jnp.where(place[:, 0][:, None] == places[None, :], route_weights[:, 0][:, None], 0.0)
    mix = low + jnp.where(place[:, 1][:, None] == places[None, :], route_weights[:, 1][:, None], 0.0)
    mix_high, mix_low = split(mix)

    cuts_first = call(cut_first, [shape(1024, 256)] * 3, where, w_gate[0], w_up[0], flops=2**22, vmem=LARGE)
    cuts_second = call(cut_second, [shape(512, 256)] * 3, where, w_down[0], flops=2**21, vmem=LARGE)

    cut_theirs = call(cut_out, [shape(1024, cols)], where, out_weight, flops=2**20, vmem=LARGE)
    theirs = lax.ppermute(cut_theirs, PLANE, PARTNERS)
    pooled_half = a2a(pooled, HALVES)
    mine, other = call(
        project,
        [shape(length, cols, dtype=F32), shape(length, cols)],
        where,
        pooled_half,
        out_weight,
        theirs,
        residual,
        flops=2**29,
    )
    received = lax.ppermute(other, PLANE, PARTNERS)
    updated, send = call(
        finish, [shape(length, cols), shape(slots, cols)], mine, received, place.T, flops=2**27, tables=0
    )
    arrived = lax.all_to_all(send.reshape(n_exp, cap, cols), SP, 0, 0, tiled=True).reshape(slots, cols)
    first = [w_gate[0], w_up[0], *turns(cuts_first, SCATTER)]
    second = [w_down[0], *turns(cuts_second, GATHER)]
    made = experts(arrived, first, second, where, norm_gain.reshape(16, 256))
    back = lax.all_to_all(made.reshape(n_exp, cap, cols), SP, 0, 0, tiled=True).reshape(slots, cols)
    summed = jnp.dot(mix_high, back, preferred_element_type=F32) + jnp.dot(
        mix_low, back, preferred_element_type=F32
    )
    return (updated.astype(F32) + summed).astype(BF16)


def solution(mesh):
    torus = Mesh(mesh.devices.reshape(-1, 2, 4, 4), ("z", *PLANE))
    in_specs = (
        P(SP, TP),
        P(SP, TP),
        P(SP),
        P(TP, None, None),
        P(TP),
        P(None, TP),
        P(),
        P(SP, None),
        P(SP, None),
        P(SP, None, TP),
        P(SP, None, TP),
        P(SP, None, TP),
    )
    return jax.shard_map(layer, mesh=torus, in_specs=in_specs, out_specs=P(SP, TP), check_vma=False)
```

```python
import jax
import jax.numpy as jnp
import numpy as np
from jax import lax
from jax.experimental import pallas as pl
from jax.experimental.pallas import tpu as pltpu
from jax.sharding import Mesh
from jax.sharding import PartitionSpec as P


TOPK = 2
SP = ("z", "c")
TP = ("y", "x")
PLANE = ("c", "y", "x")
EPS = 1e-06
F32 = jnp.float32
BF16 = jnp.bfloat16
VMEM_BYTES = 20 * 2**20
LARGE = 58 * 2**20


def blocks_of(shift):
    return [
        [(2 * v + shift + i) % 4 * 4 + (2 * h + shift + j) % 4 for i in (0, 1) for j in (0, 1)]
        for v in (0, 1)
        for h in (0, 1)
    ]


GATHER = [blocks_of(1), blocks_of(0)]
SCATTER = [blocks_of(0), blocks_of(1)]


def both_cores(groups):
    return groups[0] + [[16 + m for m in group] for group in groups[1]]


def group_with(groups, member):
    return next(group for group in groups if member in group)


def tables():
    table = np.zeros((2, 16, 40), np.int32)
    for core in range(2):
        for me in range(16):
            gather, scatter = group_with(GATHER[core], me), group_with(SCATTER[core], me)
            p, q = scatter.index(me), gather.index(me)
            row = []
            for by in range(4):
                row += group_with(GATHER[core], scatter[(p + by) % 4])
            for by in range(4):
                row += group_with(SCATTER[core], gather[(q + by) % 4])
            table[core, me, :39] = row + gather + [p, q, 2 ** (1 + me % 4)]
    return table


FEATURES, HIDDEN, GAINS, IN_SCATTER, IN_GATHER, SPAN, SP_INDEX = 0, 16, 32, 36, 37, 38, 39


def a2a(blocks, groups):
    return lax.all_to_all(blocks, PLANE, 0, 0, tiled=True, axis_index_groups=both_cores(groups))


def turns(cuts, groups):
    got = [cuts[0]]
    for by in range(1, 4):
        pairs = [(g[i], g[(i + by) % 4]) for g in both_cores(groups) for i in range(4)]
        got.append(lax.ppermute(cuts[by], PLANE, pairs))
    return got


def shape(*dims, dtype=BF16):
    return jax.ShapeDtypeStruct(dims, dtype)


def call(kernel, outs, *args, flops, scratch=(), vmem=VMEM_BYTES, tables=1):
    single = len(outs) == 1
    moved = sum(a.size * a.dtype.itemsize for a in (*args, *outs))
    whole = pl.BlockSpec(memory_space=pltpu.VMEM)
    specs = [pl.BlockSpec(memory_space=pltpu.SMEM)] * tables
    specs += [whole] * (len(args) - tables)
    return pl.pallas_call(
        kernel,
        out_shape=outs[0] if single else tuple(outs),
        in_specs=specs,
        out_specs=whole if single else (whole,) * len(outs),
        scratch_shapes=list(scratch),
        compiler_params=pltpu.CompilerParams(vmem_limit_bytes=vmem),
        cost_estimate=pl.CostEstimate(flops=flops, bytes_accessed=moved, transcendentals=0),
    )(*args)


def cut_first(where, gate, up, *outs):
    for by in range(4):
        for i in range(4):
            block = where[FEATURES + 4 * by + i]
            src = pl.ds(pl.multiple_of(block * 256, 256), 256)
            outs[by][pl.ds(256 * i, 256), pl.ds(0, 128)] = gate[src, :]
            outs[by][pl.ds(256 * i, 256), pl.ds(128, 128)] = up[src, :]


def cut_second(where, down, *outs):
    for by in range(4):
        for i in range(4):
            block = where[HIDDEN + 4 * by + i]
            outs[by][pl.ds(128 * i, 128), :] = down[pl.ds(pl.multiple_of(block * 128, 128), 128), :]


def pack(where, w0, w1, w2, w3, out):
    for by, block in enumerate((w0, w1, w2, w3)):
        out[lax.rem(where[IN_SCATTER] + 4 - by, 4)] = block[...]


def gate_up(where, got, gain, first, out, rows):
    count = got.shape[1]
    ones = jnp.ones((8, 256), BF16)
    tiles = count // 256
    for i in range(tiles):
        tile = pl.ds(256 * i, 256)
        total = jnp.zeros((8, 256), F32)
        for g in range(4):
            value = got[g, tile, :].astype(F32)
            for h in range(2):
                scaled = value[:, 128 * h : 128 * h + 128] * gain[pl.ds(2 * where[GAINS + g] + h, 1), :]
                rows[tile, pl.ds(256 * g + 128 * h, 128)] = scaled.astype(BF16)
            square = value * value
            high = square.astype(BF16)
            low = (square - high.astype(F32)).astype(BF16)
            for part in (high, low):
                total = total + lax.dot_general(ones, part, (((1,), (1,)), ((), ())), preferred_element_type=F32)
        high = total.astype(BF16)
        low = (total - high.astype(F32)).astype(BF16)
        for j in range(4):
            out[j, pl.ds(count + 2 * i, 1), :] = high[:1]
            out[j, pl.ds(count + 2 * i + 1, 1), :] = low[:1]
    for to in range(4):
        out[to, pl.ds(count + 2 * tiles, 8 - 2 * tiles), :] = jnp.zeros((8 - 2 * tiles, 256), BF16)
        for i in range(tiles):
            tile = pl.ds(256 * i, 256)
            out[to, tile, :] = jnp.dot(rows[tile, :], first[to], preferred_element_type=F32).astype(BF16)


def activate(parts, out):
    count = out.shape[1]
    extra = jnp.concatenate([parts[j, pl.ds(count, 8), :].astype(F32) for j in range(4)], axis=0)
    line = lax.broadcasted_iota(jnp.int32, (32, 128), 0) % 8
    for i in range(count // 256):
        tile = pl.ds(256 * i, 256)
        pick = ((line == 2 * i) | (line == 2 * i + 1)).astype(F32)
        total = lax.dot_general(extra, pick, (((0,), (0,)), ((), ())), preferred_element_type=F32)
        scale = lax.rsqrt(total / 4096 + EPS)
        gate = parts[0, tile, pl.ds(0, 128)].astype(F32)
        up = parts[0, tile, pl.ds(128, 128)].astype(F32)
        for j in range(1, 4):
            gate = gate + parts[j, tile, pl.ds(0, 128)].astype(F32)
            up = up + parts[j, tile, pl.ds(128, 128)].astype(F32)
        gate, up = gate * scale, up * scale
        act = (gate * jax.nn.sigmoid(gate) * up).astype(BF16)
        for j in range(4):
            out[j, tile, :] = act


def down_rows(where, acts, w0, w1, w2, w3, out, rows):
    count = acts.shape[1]
    for h in range(4):
        rows[:, pl.ds(128 * h, 128)] = acts[h]
    for by, second in enumerate((w0, w1, w2, w3)):
        to = lax.rem(where[IN_GATHER] + 4 - by, 4)
        for i in range(count // 256):
            tile = pl.ds(256 * i, 256)
            out[to, tile, :] = jnp.dot(rows[tile, :], second[...], preferred_element_type=F32).astype(BF16)


def experts(arrived, first, second, where, gain):
    count = arrived.shape[0]
    got = a2a(jnp.broadcast_to(arrived[None], (4, *arrived.shape)), GATHER)
    part = call(
        gate_up,
        [shape(4, count + 8, 256)],
        where,
        got,
        gain,
        first,
        flops=2**21 * count,
        scratch=[pltpu.VMEM((count, 1024), BF16)],
    )
    parts = a2a(part, SCATTER)
    acts = a2a(call(activate, [shape(4, count, 128)], parts, flops=2**16 * count, tables=0), SCATTER)
    part = call(
        down_rows,
        [shape(4, count, 256)],
        where,
        acts,
        *second,
        flops=2**20 * count,
        scratch=[pltpu.VMEM((count, 512), BF16)],
    )
    parts = a2a(part, GATHER)
    return jnp.sum(parts.astype(F32), axis=0).astype(BF16)


def pool(where, own, before, docs, docs_before, weight, gain, out, extended):
    length, width = own.shape
    sp_index, span = where[SP_INDEX], where[SPAN]
    extended[pl.ds(0, 16), :] = before[pl.ds(length - 16, 16), :].astype(F32)
    extended[pl.ds(16, length), :] = own[...].astype(F32)
    now = docs[...].astype(F32)
    earlier = jnp.where(sp_index == 0, -1.0, docs_before[:, pl.ds(length - 128, 128)].astype(F32))
    line = jnp.broadcast_to(jnp.concatenate([earlier, now], axis=1), (8, length + 128))
    count = jnp.ones((8, length), F32)
    for offset in range(1, 16):
        count = count + (pltpu.roll(line, offset, 1)[:, 128:] == line[:, 128:]).astype(F32)
    eighth = jnp.full((8, width), 0.125, F32)
    count = lax.dot_general(count, eighth, (((0,), (0,)), ((), ())), preferred_element_type=F32)
    count = jnp.minimum(count, span.astype(F32))
    values = own[...].astype(F32)
    totals = values
    for offset in range(1, 16):
        totals = totals + jnp.where(count > offset, extended[pl.ds(16 - offset, length), :], 0.0)
    diff = (totals / count - values).astype(BF16)
    mixed = jnp.dot(diff, weight[0], preferred_element_type=F32)
    pooled = (mixed * gain[...]).astype(BF16)
    for j in range(16):
        out[j] = pooled


def split(value):
    high = lax.reduce_precision(value, 8, 7)
    return high.astype(BF16), (value - high).astype(BF16)


def layer(
    residual, pool_in, docs, pool_weight, pool_gain, out_weight, norm_gain, routes, route_weights, w_gate, w_up, w_down
):
    length, cols = residual.shape
    n_exp = lax.axis_size(SP)
    cap = length * TOPK * 3 // (2 * n_exp)
    slots = n_exp * cap
    where = lax.dynamic_slice(
        jnp.asarray(tables()), (lax.axis_index("c"), lax.axis_index(TP), 0), (1, 1, 40)
    ).reshape(40)
    where = where.at[SP_INDEX].set(lax.axis_index(SP))
    onward = [(i, i + 1) for i in range(n_exp - 1)]
    before = lax.ppermute(pool_in, SP, onward)
    docs_before = lax.ppermute(docs.reshape(1, length), SP, onward)
    pooled = call(
        pool,
        [shape(16, *pool_in.shape)],
        where,
        pool_in,
        before,
        docs.reshape(1, length),
        docs_before,
        pool_weight,
        pool_gain.reshape(1, -1),
        flops=2**23,
        scratch=[pltpu.VMEM((length + 16, pool_in.shape[1]), F32)],
        vmem=LARGE,
    )
    ids = routes.reshape(-1)
    onehot = (ids[:, None] == jnp.arange(n_exp)[None, :]).astype(jnp.int32)
    rank = jnp.sum(onehot * (jnp.cumsum(onehot, axis=0) - 1), axis=1)
    place = (ids * cap + rank).reshape(length, TOPK)
    places = jnp.arange(slots)
    take = (place[:, 0][None, :] == places[:, None]) | (place[:, 1][None, :] == places[:, None])
    low = jnp.where(place[:, 0][:, None] == places[None, :], route_weights[:, 0][:, None], 0.0)
    mix = low + jnp.where(place[:, 1][:, None] == places[None, :], route_weights[:, 1][:, None], 0.0)
    mix_high, mix_low = split(mix)

    cuts_first = call(cut_first, [shape(1024, 256)] * 4, where, w_gate[0], w_up[0], flops=2**22, vmem=LARGE)
    cuts_second = call(cut_second, [shape(512, 256)] * 4, where, w_down[0], flops=2**21, vmem=LARGE)

    pooled_all = lax.all_to_all(pooled, TP, 0, 0, tiled=True)
    proj = jnp.einsum("gtc,gcd->td", pooled_all, out_weight.reshape(16, 128, cols), preferred_element_type=F32)
    updated = (residual.astype(F32) + proj).astype(BF16)

    send = jnp.dot(take.astype(BF16), updated, preferred_element_type=F32).astype(BF16)
    arrived = lax.all_to_all(send.reshape(n_exp, cap, cols), SP, 0, 0, tiled=True).reshape(slots, cols)
    first = turns(cuts_first, SCATTER)
    second = turns(cuts_second, GATHER)
    first = call(pack, [shape(4, 1024, 256)], where, *first, flops=2**22)
    made = experts(arrived, first, second, where, norm_gain.reshape(32, 128))
    back = lax.all_to_all(made.reshape(n_exp, cap, cols), SP, 0, 0, tiled=True).reshape(slots, cols)
    summed = jnp.dot(mix_high, back, preferred_element_type=F32) + jnp.dot(
        mix_low, back, preferred_element_type=F32
    )
    return (updated.astype(F32) + summed).astype(BF16)


def solution(mesh):
    torus = Mesh(mesh.devices.reshape(-1, 2, 4, 4), ("z", *PLANE))
    in_specs = (
        P(SP, TP),
        P(SP, TP),
        P(SP),
        P(TP, None, None),
        P(TP),
        P(None, TP),
        P(),
        P(SP, None),
        P(SP, None),
        P(SP, None, TP),
        P(SP, None, TP),
        P(SP, None, TP),
    )
    return jax.shard_map(layer, mesh=torus, in_specs=in_specs, out_specs=P(SP, TP), check_vma=False)
```

```python
import jax
import jax.numpy as jnp
import numpy as np
from jax import lax
from jax.experimental import pallas as pl
from jax.experimental.pallas import tpu as pltpu
from jax.sharding import Mesh
from jax.sharding import PartitionSpec as P


TOPK = 2
SP = ("z", "c")
TP = ("y", "x")
PLANE = ("c", "y", "x")
EPS = 1e-06
F32 = jnp.float32
BF16 = jnp.bfloat16
VMEM_BYTES = 20 * 2**20
LARGE = 58 * 2**20


def blocks_of(shift):
    return [
        [(2 * v + shift + i) % 4 * 4 + (2 * h + shift + j) % 4 for i in (0, 1) for j in (0, 1)]
        for v in (0, 1)
        for h in (0, 1)
    ]


GATHER = [blocks_of(1), blocks_of(0)]
SCATTER = [blocks_of(0), blocks_of(1)]


def both_cores(groups):
    return groups[0] + [[16 + m for m in group] for group in groups[1]]


def group_with(groups, member):
    return next(group for group in groups if member in group)


def tables():
    table = np.zeros((2, 16, 40), np.int32)
    for core in range(2):
        for me in range(16):
            gather, scatter = group_with(GATHER[core], me), group_with(SCATTER[core], me)
            p, q = scatter.index(me), gather.index(me)
            row = []
            for by in range(4):
                row += group_with(GATHER[core], scatter[(p + by) % 4])
            for by in range(4):
                row += group_with(SCATTER[core], gather[(q + by) % 4])
            table[core, me, :39] = row + gather + [p, q, 2 ** (1 + me % 4)]
    return table


FEATURES, HIDDEN, GAINS, IN_SCATTER, IN_GATHER, SPAN, SP_INDEX = 0, 16, 32, 36, 37, 38, 39


def a2a(blocks, groups):
    return lax.all_to_all(blocks, PLANE, 0, 0, tiled=True, axis_index_groups=both_cores(groups))


def turns(cuts, groups):
    got = [cuts[0]]
    for by in range(1, 4):
        pairs = [(g[i], g[(i + by) % 4]) for g in both_cores(groups) for i in range(4)]
        got.append(lax.ppermute(cuts[by], PLANE, pairs))
    return got


def shape(*dims, dtype=BF16):
    return jax.ShapeDtypeStruct(dims, dtype)


def call(kernel, outs, *args, flops, scratch=(), vmem=VMEM_BYTES, tables=1):
    single = len(outs) == 1
    moved = sum(a.size * a.dtype.itemsize for a in (*args, *outs))
    whole = pl.BlockSpec(memory_space=pltpu.VMEM)
    specs = [pl.BlockSpec(memory_space=pltpu.SMEM)] * tables
    specs += [whole] * (len(args) - tables)
    return pl.pallas_call(
        kernel,
        out_shape=outs[0] if single else tuple(outs),
        in_specs=specs,
        out_specs=whole if single else (whole,) * len(outs),
        scratch_shapes=list(scratch),
        compiler_params=pltpu.CompilerParams(vmem_limit_bytes=vmem),
        cost_estimate=pl.CostEstimate(flops=flops, bytes_accessed=moved, transcendentals=0),
    )(*args)


def cut_first(where, gate, up, *outs):
    for by in range(4):
        for i in range(4):
            block = where[FEATURES + 4 * by + i]
            src = pl.ds(pl.multiple_of(block * 256, 256), 256)
            outs[by][pl.ds(256 * i, 256), pl.ds(0, 128)] = gate[src, :]
            outs[by][pl.ds(256 * i, 256), pl.ds(128, 128)] = up[src, :]


def cut_second(where, down, *outs):
    for by in range(4):
        for i in range(4):
            block = where[HIDDEN + 4 * by + i]
            outs[by][pl.ds(128 * i, 128), :] = down[pl.ds(pl.multiple_of(block * 128, 128), 128), :]


def pack(where, w0, w1, w2, w3, out):
    for by, block in enumerate((w0, w1, w2, w3)):
        out[lax.rem(where[IN_SCATTER] + 4 - by, 4)] = block[...]


def gate_up(where, got, gain, first, out, rows):
    count = got.shape[1]
    ones = jnp.ones((8, 256), BF16)
    tiles = count // 256
    for i in range(tiles):
        tile = pl.ds(256 * i, 256)
        squares = jnp.zeros((256, 256), F32)
        for g in range(4):
            value = got[g, tile, :].astype(F32)
            for h in range(2):
                scaled = value[:, 128 * h : 128 * h + 128] * gain[pl.ds(2 * where[GAINS + g] + h, 1), :]
                rows[tile, pl.ds(256 * g + 128 * h, 128)] = scaled.astype(BF16)
            squares = squares + value * value
        high = squares.astype(BF16)
        low = (squares - high.astype(F32)).astype(BF16)
        total = jnp.zeros((8, 256), F32)
        for part in (high, low):
            total = total + lax.dot_general(ones, part, (((1,), (1,)), ((), ())), preferred_element_type=F32)
        high = total.astype(BF16)
        low = (total - high.astype(F32)).astype(BF16)
        for j in range(4):
            out[j, pl.ds(count + 2 * i, 1), :] = high[:1]
            out[j, pl.ds(count + 2 * i + 1, 1), :] = low[:1]
    for to in range(4):
        out[to, pl.ds(count + 2 * tiles, 8 - 2 * tiles), :] = jnp.zeros((8 - 2 * tiles, 256), BF16)
        for i in range(tiles):
            tile = pl.ds(256 * i, 256)
            out[to, tile, :] = jnp.dot(rows[tile, :], first[to], preferred_element_type=F32).astype(BF16)


def activate(parts, out):
    count = out.shape[1]
    extra = jnp.concatenate([parts[j, pl.ds(count, 8), :].astype(F32) for j in range(4)], axis=0)
    line = lax.broadcasted_iota(jnp.int32, (32, 128), 0) % 8
    for i in range(count // 256):
        tile = pl.ds(256 * i, 256)
        pick = ((line == 2 * i) | (line == 2 * i + 1)).astype(F32)
        total = lax.dot_general(extra, pick, (((0,), (0,)), ((), ())), preferred_element_type=F32)
        scale = lax.rsqrt(total / 4096 + EPS)
        gate = parts[0, tile, pl.ds(0, 128)].astype(F32)
        up = parts[0, tile, pl.ds(128, 128)].astype(F32)
        for j in range(1, 4):
            gate = gate + parts[j, tile, pl.ds(0, 128)].astype(F32)
            up = up + parts[j, tile, pl.ds(128, 128)].astype(F32)
        gate, up = gate * scale, up * scale
        act = (gate * jax.nn.sigmoid(gate) * up).astype(BF16)
        for j in range(4):
            out[j, tile, :] = act


def down_rows(where, acts, w0, w1, w2, w3, out, rows):
    count = acts.shape[1]
    for h in range(4):
        rows[:, pl.ds(128 * h, 128)] = acts[h]
    for by, second in enumerate((w0, w1, w2, w3)):
        to = lax.rem(where[IN_GATHER] + 4 - by, 4)
        for i in range(count // 256):
            tile = pl.ds(256 * i, 256)
            out[to, tile, :] = jnp.dot(rows[tile, :], second[...], preferred_element_type=F32).astype(BF16)


def experts(arrived, first, second, where, gain):
    count = arrived.shape[0]
    got = a2a(jnp.broadcast_to(arrived[None], (4, *arrived.shape)), GATHER)
    part = call(
        gate_up,
        [shape(4, count + 8, 256)],
        where,
        got,
        gain,
        first,
        flops=2**21 * count,
        scratch=[pltpu.VMEM((count, 1024), BF16)],
    )
    parts = a2a(part, SCATTER)
    acts = a2a(call(activate, [shape(4, count, 128)], parts, flops=2**16 * count, tables=0), SCATTER)
    part = call(
        down_rows,
        [shape(4, count, 256)],
        where,
        acts,
        *second,
        flops=2**20 * count,
        scratch=[pltpu.VMEM((count, 512), BF16)],
    )
    parts = a2a(part, GATHER)
    return jnp.sum(parts.astype(F32), axis=0).astype(BF16)


def pool(where, own, before, docs, docs_before, weight, gain, out, extended):
    length, width = own.shape
    sp_index, span = where[SP_INDEX], where[SPAN]
    extended[pl.ds(0, 16), :] = before[pl.ds(length - 16, 16), :].astype(F32)
    extended[pl.ds(16, length), :] = own[...].astype(F32)
    now = docs[...].astype(F32)
    earlier = jnp.where(sp_index == 0, -1.0, docs_before[:, pl.ds(length - 128, 128)].astype(F32))
    line = jnp.broadcast_to(jnp.concatenate([earlier, now], axis=1), (8, length + 128))
    count = jnp.ones((8, length), F32)
    for offset in range(1, 16):
        count = count + (pltpu.roll(line, offset, 1)[:, 128:] == line[:, 128:]).astype(F32)
    eighth = jnp.full((8, width), 0.125, F32)
    count = lax.dot_general(count, eighth, (((0,), (0,)), ((), ())), preferred_element_type=F32)
    count = jnp.minimum(count, span.astype(F32))
    values = own[...].astype(F32)
    totals = values
    for offset in range(1, 16):
        totals = totals + jnp.where(count > offset, extended[pl.ds(16 - offset, length), :], 0.0)
    diff = (totals / count - values).astype(BF16)
    mixed = jnp.dot(diff, weight[0], preferred_element_type=F32)
    pooled = (mixed * gain[...]).astype(BF16)
    for j in range(16):
        out[j] = pooled


def split(value):
    high = lax.reduce_precision(value, 8, 7)
    return high.astype(BF16), (value - high).astype(BF16)


def layer(
    residual, pool_in, docs, pool_weight, pool_gain, out_weight, norm_gain, routes, route_weights, w_gate, w_up, w_down
):
    length, cols = residual.shape
    n_exp = lax.axis_size(SP)
    cap = length * TOPK * 3 // (2 * n_exp)
    slots = n_exp * cap
    where = lax.dynamic_slice(
        jnp.asarray(tables()), (lax.axis_index("c"), lax.axis_index(TP), 0), (1, 1, 40)
    ).reshape(40)
    where = where.at[SP_INDEX].set(lax.axis_index(SP))
    onward = [(i, i + 1) for i in range(n_exp - 1)]
    before = lax.ppermute(pool_in, SP, onward)
    docs_before = lax.ppermute(docs.reshape(1, length), SP, onward)
    pooled = call(
        pool,
        [shape(16, *pool_in.shape)],
        where,
        pool_in,
        before,
        docs.reshape(1, length),
        docs_before,
        pool_weight,
        pool_gain.reshape(1, -1),
        flops=2**23,
        scratch=[pltpu.VMEM((length + 16, pool_in.shape[1]), F32)],
        vmem=LARGE,
    )
    ids = routes.reshape(-1)
    onehot = (ids[:, None] == jnp.arange(n_exp)[None, :]).astype(jnp.int32)
    rank = jnp.sum(onehot * (jnp.cumsum(onehot, axis=0) - 1), axis=1)
    place = (ids * cap + rank).reshape(length, TOPK)
    places = jnp.arange(slots)
    take = (place[:, 0][None, :] == places[:, None]) | (place[:, 1][None, :] == places[:, None])
    low = jnp.where(place[:, 0][:, None] == places[None, :], route_weights[:, 0][:, None], 0.0)
    mix = low + jnp.where(place[:, 1][:, None] == places[None, :], route_weights[:, 1][:, None], 0.0)
    mix_high, mix_low = lax.optimization_barrier(split(mix))

    cuts_first = call(cut_first, [shape(1024, 256)] * 4, where, w_gate[0], w_up[0], flops=2**22, vmem=LARGE)
    cuts_second = call(cut_second, [shape(512, 256)] * 4, where, w_down[0], flops=2**21, vmem=LARGE)

    pooled_all = lax.all_to_all(pooled, TP, 0, 0, tiled=True)
    proj = jnp.einsum("gtc,gcd->td", pooled_all, out_weight.reshape(16, 128, cols), preferred_element_type=F32)
    updated = (residual.astype(F32) + proj).astype(BF16)

    send = jnp.dot(lax.optimization_barrier(take.astype(BF16)), updated, preferred_element_type=F32).astype(BF16)
    arrived = lax.all_to_all(send.reshape(n_exp, cap, cols), SP, 0, 0, tiled=True).reshape(slots, cols)
    first = turns(cuts_first, SCATTER)
    second = turns(cuts_second, GATHER)
    first = call(pack, [shape(4, 1024, 256)], where, *first, flops=2**22)
    made = experts(arrived, first, second, where, norm_gain.reshape(32, 128))
    back = lax.all_to_all(made.reshape(n_exp, cap, cols), SP, 0, 0, tiled=True).reshape(slots, cols)
    summed = jnp.dot(mix_high, back, preferred_element_type=F32) + jnp.dot(
        mix_low, back, preferred_element_type=F32
    )
    return (updated.astype(F32) + summed).astype(BF16)


def solution(mesh):
    torus = Mesh(mesh.devices.reshape(-1, 2, 4, 4), ("z", *PLANE))
    in_specs = (
        P(SP, TP),
        P(SP, TP),
        P(SP),
        P(TP, None, None),
        P(TP),
        P(None, TP),
        P(),
        P(SP, None),
        P(SP, None),
        P(SP, None, TP),
        P(SP, None, TP),
        P(SP, None, TP),
    )
    return jax.shard_map(layer, mesh=torus, in_specs=in_specs, out_specs=P(SP, TP), check_vma=False)
```

```python
import jax
import jax.numpy as jnp
import numpy as np
from jax import lax
from jax.experimental import pallas as pl
from jax.experimental.pallas import tpu as pltpu
from jax.sharding import Mesh
from jax.sharding import PartitionSpec as P


TOPK = 2
SP = ("z", "c")
TP = ("y", "x")
PLANE = ("c", "y", "x")
EPS = 1e-06
F32 = jnp.float32
BF16 = jnp.bfloat16
VMEM_BYTES = 20 * 2**20
LARGE = 58 * 2**20


def blocks_of(shift):
    return [
        [(2 * v + shift + i) % 4 * 4 + (2 * h + shift + j) % 4 for i in (0, 1) for j in (0, 1)]
        for v in (0, 1)
        for h in (0, 1)
    ]


GATHER = [blocks_of(1), blocks_of(0)]
SCATTER = [blocks_of(0), blocks_of(1)]


def both_cores(groups):
    return groups[0] + [[16 + m for m in group] for group in groups[1]]


def group_with(groups, member):
    return next(group for group in groups if member in group)


def tables():
    table = np.zeros((2, 16, 40), np.int32)
    for core in range(2):
        for me in range(16):
            gather, scatter = group_with(GATHER[core], me), group_with(SCATTER[core], me)
            p, q = scatter.index(me), gather.index(me)
            row = []
            for by in range(4):
                row += group_with(GATHER[core], scatter[(p + by) % 4])
            for by in range(4):
                row += group_with(SCATTER[core], gather[(q + by) % 4])
            table[core, me, :39] = row + gather + [p, q, 2 ** (1 + me % 4)]
    return table


FEATURES, HIDDEN, GAINS, IN_SCATTER, IN_GATHER, SPAN, SP_INDEX = 0, 16, 32, 36, 37, 38, 39


def a2a(blocks, groups):
    return lax.all_to_all(blocks, PLANE, 0, 0, tiled=True, axis_index_groups=both_cores(groups))


FIRST = 24


def exchanged(blocks):
    size = blocks.shape[0]
    order = [(FIRST + i) % size for i in range(size)]
    return lax.all_to_all(blocks, SP, 0, 0, tiled=True, axis_index_groups=[order])


def turns(cuts, groups):
    got = [cuts[0]]
    for by in range(1, 4):
        pairs = [(g[i], g[(i + by) % 4]) for g in both_cores(groups) for i in range(4)]
        got.append(lax.ppermute(cuts[by], PLANE, pairs))
    return got


def shape(*dims, dtype=BF16):
    return jax.ShapeDtypeStruct(dims, dtype)


def call(kernel, outs, *args, flops, scratch=(), vmem=VMEM_BYTES, tables=1):
    single = len(outs) == 1
    moved = sum(a.size * a.dtype.itemsize for a in (*args, *outs))
    whole = pl.BlockSpec(memory_space=pltpu.VMEM)
    specs = [pl.BlockSpec(memory_space=pltpu.SMEM)] * tables
    specs += [whole] * (len(args) - tables)
    return pl.pallas_call(
        kernel,
        out_shape=outs[0] if single else tuple(outs),
        in_specs=specs,
        out_specs=whole if single else (whole,) * len(outs),
        scratch_shapes=list(scratch),
        compiler_params=pltpu.CompilerParams(vmem_limit_bytes=vmem),
        cost_estimate=pl.CostEstimate(flops=flops, bytes_accessed=moved, transcendentals=0),
    )(*args)


def cut_first(where, gate, up, *outs):
    for by in range(4):
        for i in range(4):
            block = where[FEATURES + 4 * by + i]
            src = pl.ds(pl.multiple_of(block * 256, 256), 256)
            outs[by][pl.ds(256 * i, 256), pl.ds(0, 128)] = gate[src, :]
            outs[by][pl.ds(256 * i, 256), pl.ds(128, 128)] = up[src, :]


def cut_second(where, down, *outs):
    for by in range(4):
        for i in range(4):
            block = where[HIDDEN + 4 * by + i]
            outs[by][pl.ds(128 * i, 128), :] = down[pl.ds(pl.multiple_of(block * 128, 128), 128), :]


def pack(where, w0, w1, w2, w3, out):
    for by, block in enumerate((w0, w1, w2, w3)):
        out[lax.rem(where[IN_SCATTER] + 4 - by, 4)] = block[...]


def gate_up(where, got, gain, first, out, rows):
    count = got.shape[1]
    ones = jnp.ones((8, 256), BF16)
    tiles = count // 256
    for i in range(tiles):
        tile = pl.ds(256 * i, 256)
        squares = jnp.zeros((256, 256), F32)
        for g in range(4):
            value = got[g, tile, :].astype(F32)
            for h in range(2):
                scaled = value[:, 128 * h : 128 * h + 128] * gain[pl.ds(2 * where[GAINS + g] + h, 1), :]
                rows[tile, pl.ds(256 * g + 128 * h, 128)] = scaled.astype(BF16)
            squares = squares + value * value
        high = squares.astype(BF16)
        low = (squares - high.astype(F32)).astype(BF16)
        total = jnp.zeros((8, 256), F32)
        for part in (high, low):
            total = total + lax.dot_general(ones, part, (((1,), (1,)), ((), ())), preferred_element_type=F32)
        high = total.astype(BF16)
        low = (total - high.astype(F32)).astype(BF16)
        for j in range(4):
            out[j, pl.ds(count + 2 * i, 1), :] = high[:1]
            out[j, pl.ds(count + 2 * i + 1, 1), :] = low[:1]
    for to in range(4):
        out[to, pl.ds(count + 2 * tiles, 8 - 2 * tiles), :] = jnp.zeros((8 - 2 * tiles, 256), BF16)
        for i in range(tiles):
            tile = pl.ds(256 * i, 256)
            out[to, tile, :] = jnp.dot(rows[tile, :], first[to], preferred_element_type=F32).astype(BF16)


def activate(parts, out):
    count = out.shape[1]
    extra = jnp.concatenate([parts[j, pl.ds(count, 8), :].astype(F32) for j in range(4)], axis=0)
    line = lax.broadcasted_iota(jnp.int32, (32, 128), 0) % 8
    for i in range(count // 256):
        tile = pl.ds(256 * i, 256)
        pick = ((line == 2 * i) | (line == 2 * i + 1)).astype(F32)
        total = lax.dot_general(extra, pick, (((0,), (0,)), ((), ())), preferred_element_type=F32)
        scale = lax.rsqrt(total / 4096 + EPS)
        gate = parts[0, tile, pl.ds(0, 128)].astype(F32)
        up = parts[0, tile, pl.ds(128, 128)].astype(F32)
        for j in range(1, 4):
            gate = gate + parts[j, tile, pl.ds(0, 128)].astype(F32)
            up = up + parts[j, tile, pl.ds(128, 128)].astype(F32)
        gate, up = gate * scale, up * scale
        act = (gate * jax.nn.sigmoid(gate) * up).astype(BF16)
        for j in range(4):
            out[j, tile, :] = act


def down_rows(where, acts, w0, w1, w2, w3, out, rows):
    count = acts.shape[1]
    for h in range(4):
        rows[:, pl.ds(128 * h, 128)] = acts[h]
    for by, second in enumerate((w0, w1, w2, w3)):
        to = lax.rem(where[IN_GATHER] + 4 - by, 4)
        for i in range(count // 256):
            tile = pl.ds(256 * i, 256)
            out[to, tile, :] = jnp.dot(rows[tile, :], second[...], preferred_element_type=F32).astype(BF16)


def experts(arrived, first, second, where, gain):
    count = arrived.shape[0]
    got = a2a(jnp.broadcast_to(arrived[None], (4, *arrived.shape)), GATHER)
    part = call(
        gate_up,
        [shape(4, count + 8, 256)],
        where,
        got,
        gain,
        first,
        flops=2**21 * count,
        scratch=[pltpu.VMEM((count, 1024), BF16)],
    )
    parts = a2a(part, SCATTER)
    acts = a2a(call(activate, [shape(4, count, 128)], parts, flops=2**16 * count, tables=0), SCATTER)
    part = call(
        down_rows,
        [shape(4, count, 256)],
        where,
        acts,
        *second,
        flops=2**20 * count,
        scratch=[pltpu.VMEM((count, 512), BF16)],
    )
    parts = a2a(part, GATHER)
    return jnp.sum(parts.astype(F32), axis=0).astype(BF16)


def pool(where, own, before, docs, docs_before, weight, gain, out, extended):
    length, width = own.shape
    sp_index, span = where[SP_INDEX], where[SPAN]
    extended[pl.ds(0, 16), :] = before[pl.ds(length - 16, 16), :].astype(F32)
    extended[pl.ds(16, length), :] = own[...].astype(F32)
    now = docs[...].astype(F32)
    earlier = jnp.where(sp_index == 0, -1.0, docs_before[:, pl.ds(length - 128, 128)].astype(F32))
    line = jnp.broadcast_to(jnp.concatenate([earlier, now], axis=1), (8, length + 128))
    count = jnp.ones((8, length), F32)
    for offset in range(1, 16):
        count = count + (pltpu.roll(line, offset, 1)[:, 128:] == line[:, 128:]).astype(F32)
    eighth = jnp.full((8, width), 0.125, F32)
    count = lax.dot_general(count, eighth, (((0,), (0,)), ((), ())), preferred_element_type=F32)
    count = jnp.minimum(count, span.astype(F32))
    values = own[...].astype(F32)
    totals = values
    for offset in range(1, 16):
        totals = totals + jnp.where(count > offset, extended[pl.ds(16 - offset, length), :], 0.0)
    diff = (totals / count - values).astype(BF16)
    mixed = jnp.dot(diff, weight[0], preferred_element_type=F32)
    pooled = (mixed * gain[...]).astype(BF16)
    for j in range(16):
        out[j] = pooled


def split(value):
    high = lax.reduce_precision(value, 8, 7)
    return high.astype(BF16), (value - high).astype(BF16)


def layer(
    residual, pool_in, docs, pool_weight, pool_gain, out_weight, norm_gain, routes, route_weights, w_gate, w_up, w_down
):
    length, cols = residual.shape
    n_exp = lax.axis_size(SP)
    cap = length * TOPK * 3 // (2 * n_exp)
    slots = n_exp * cap
    where = lax.dynamic_slice(
        jnp.asarray(tables()), (lax.axis_index("c"), lax.axis_index(TP), 0), (1, 1, 40)
    ).reshape(40)
    where = where.at[SP_INDEX].set(lax.axis_index(SP))
    onward = [(i, i + 1) for i in range(n_exp - 1)]
    before = lax.ppermute(pool_in, SP, onward)
    docs_before = lax.ppermute(docs.reshape(1, length), SP, onward)
    pooled = call(
        pool,
        [shape(16, *pool_in.shape)],
        where,
        pool_in,
        before,
        docs.reshape(1, length),
        docs_before,
        pool_weight,
        pool_gain.reshape(1, -1),
        flops=2**23,
        scratch=[pltpu.VMEM((length + 16, pool_in.shape[1]), F32)],
        vmem=LARGE,
    )
    ids = routes.reshape(-1)
    onehot = (ids[:, None] == jnp.arange(n_exp)[None, :]).astype(jnp.int32)
    rank = jnp.sum(onehot * (jnp.cumsum(onehot, axis=0) - 1), axis=1)
    place = ((ids + (n_exp - FIRST)) % n_exp * cap + rank).reshape(length, TOPK)
    places = jnp.arange(slots)
    take = (place[:, 0][None, :] == places[:, None]) | (place[:, 1][None, :] == places[:, None])
    low = jnp.where(place[:, 0][:, None] == places[None, :], route_weights[:, 0][:, None], 0.0)
    mix = low + jnp.where(place[:, 1][:, None] == places[None, :], route_weights[:, 1][:, None], 0.0)
    mix_high, mix_low = lax.optimization_barrier(split(mix))

    cuts_first = call(cut_first, [shape(1024, 256)] * 4, where, w_gate[0], w_up[0], flops=2**22, vmem=LARGE)
    cuts_second = call(cut_second, [shape(512, 256)] * 4, where, w_down[0], flops=2**21, vmem=LARGE)

    pooled_all = lax.all_to_all(pooled, TP, 0, 0, tiled=True)
    proj = jnp.einsum("gtc,gcd->td", pooled_all, out_weight.reshape(16, 128, cols), preferred_element_type=F32)
    updated = (residual.astype(F32) + proj).astype(BF16)

    send = jnp.dot(lax.optimization_barrier(take.astype(BF16)), updated, preferred_element_type=F32).astype(BF16)
    arrived = exchanged(send.reshape(n_exp, cap, cols)).reshape(slots, cols)
    first = turns(cuts_first, SCATTER)
    second = turns(cuts_second, GATHER)
    first = call(pack, [shape(4, 1024, 256)], where, *first, flops=2**22)
    made = experts(arrived, first, second, where, norm_gain.reshape(32, 128))
    back = exchanged(made.reshape(n_exp, cap, cols)).reshape(slots, cols)
    summed = jnp.dot(mix_high, back, preferred_element_type=F32) + jnp.dot(
        mix_low, back, preferred_element_type=F32
    )
    return (updated.astype(F32) + summed).astype(BF16)


def solution(mesh):
    torus = Mesh(mesh.devices.reshape(-1, 2, 4, 4), ("z", *PLANE))
    in_specs = (
        P(SP, TP),
        P(SP, TP),
        P(SP),
        P(TP, None, None),
        P(TP),
        P(None, TP),
        P(),
        P(SP, None),
        P(SP, None),
        P(SP, None, TP),
        P(SP, None, TP),
        P(SP, None, TP),
    )
    return jax.shard_map(layer, mesh=torus, in_specs=in_specs, out_specs=P(SP, TP), check_vma=False)
```
